32 devices in a mesh: ep: 4 (over z), tp: 8 (over y, x, core).
Axes of the slice: x: 2, y: 2, z: 4, core: 2. Of those that a mesh axis runs over, the one named last changes fastest.
Arguments:
- tokens: bfloat16 [1024, 2048], P('ep'), may hold values from -6 to 6
- norm_gain: float32 [2048], replicated, may hold values from 0.1 to 1.9
- expert_ids: int32 [1024, 2], P('ep'), may hold values from 0 to 3, all different within a row; in each aligned block of 256 rows (0 to 255, 256 to 511, ...) at most 192 rows name the same one
- routing_weight: float32 [1024, 2], P('ep'), may hold values from 0.1 to 1
- expert_gate: bfloat16 [4, 2048, 5632], P('ep', None, 'tp'), may hold values from -0.125 to 0.125
- expert_up: bfloat16 [4, 2048, 5632], P('ep', None, 'tp'), may hold values from -0.125 to 0.125
- expert_down: bfloat16 [4, 5632, 2048], P('ep', 'tp'), may hold values from -0.078125 to 0.078125
- dense_gate_w: bfloat16 [2048, 1024], P(None, 'tp'), may hold values from -0.125 to 0.125
- dense_up_w: bfloat16 [2048, 1024], P(None, 'tp'), may hold values from -0.125 to 0.125
- dense_down_w: bfloat16 [1024, 2048], P('tp'), may hold values from -0.1875 to 0.1875
- dense_gate: float32 [2048], P('tp'), may hold values from -3 to 3
Outputs:
- layer_out: bfloat16 [1024, 2048], P('ep', 'tp')
The draws below stay inside these ranges and needn't reach their ends.
Inputs may be any that keep to these rules, and one draw needn't show every extreme that they name: `expert_ids`: within the 256 rows of one device along ep, each row names two different experts and no expert is named by more than 192 rows; some expert is named by exactly 192 rows.
All inputs are finite; a program needn't handle non-finite values.
Results may differ from the reference program's by a relative error of at most 0.017.
Values may be sent and summed in bfloat16 or wider, within the bound.
A program may use at most 64 MiB of HBM per device.

```python
import math
import jax
import jax.numpy as jnp
import numpy as np
from jax import lax

D = 2048
FF = 5632
DS = 1024
TOK_G = 256
EXPERTS = 4
CAP = 192
TOKENS = 1024
FF_PART = 704
DS_PART = 128
N_EP = 4
N_TP = 8


def block_levels(stream_key, dims, cuts, least, high):
    loudness, own = 1.0, jax.random.fold_in(stream_key, 6)
    for position, parts in cuts:
        steps = jnp.exp(jax.random.uniform(jax.random.fold_in(own, position), (parts,), jnp.float32, least / len(cuts), high / len(cuts)))
        loudness = loudness * jnp.repeat(steps, dims[position] // parts).reshape([-1 if axis == position else 1 for axis in range(len(dims))])
    return loudness


def shared_out(stream_key, own, number, rows, number_of, top, most, slope):
    order = jax.random.permutation(stream_key, number_of)
    packed, usual = portions_of(number_of, rows * top, most, slope, True), portions_of(number_of, rows * top, most, slope, False)
    places = jnp.arange(number_of)

    def named(lengths, offset_by):
        used = int((lengths > 0).sum())
        fixed = max(1, used // 4)
        shifted = fixed + (places - fixed + offset_by * (used - fixed)) % max(1, number_of - fixed)
        return jnp.zeros((number_of,), jnp.int32).at[order[jnp.where(places < fixed, places, shifted)]].set(jnp.asarray(lengths, jnp.int32))

    lengths = jnp.where(number % 4 == 0, named(packed, number // 4), named(usual, number - number // 4 - 1))
    mixed = jax.random.permutation(jax.random.fold_in(own, 3), number_of)
    donor, receiver = mixed[0:number_of // 2 * 2:2], mixed[1:number_of // 2 * 2:2]
    margin = jnp.minimum(lengths[donor] - 1, most - lengths[receiver]) // 2
    margin = jnp.where((donor == order[0]) | (receiver == order[0]) | (lengths[receiver] == 0), 0, jnp.maximum(margin, 0))
    shifted = jax.random.randint(jax.random.fold_in(own, 4), (number_of // 2,), 0, 1 << 20) % (margin + 1)
    lengths = lengths.at[donor].add(-shifted).at[receiver].add(shifted)
    labels = jnp.searchsorted(jnp.cumsum(lengths), jnp.arange(rows * top), side="right").astype(jnp.int32)
    table = labels.reshape(top, rows).T
    table = table[jax.random.permutation(jax.random.fold_in(own, 1), rows)]
    offset_by = jax.random.randint(jax.random.fold_in(own, 2), (rows, 1), 0, top)
    return jnp.take_along_axis(table, (jnp.arange(top)[None, :] + offset_by) % top, axis=1)


def portions_of(number_of, total, reach, skew, full):
    weights = [(1 << 20) // math.isqrt(standing ** skew) + 1 for standing in range(1, number_of + 1)]
    largest = reach if full else min(reach, max(-(-total // number_of), total * weights[0] // sum(weights)))
    least = 1 if total - largest >= number_of - 1 else 0
    given, rest = [largest] + [least] * (number_of - 1), total - largest - least * (number_of - 1)
    while rest > 0:
        free = [i for i in range(1, number_of) if given[i] < largest] or [i for i in range(1, number_of) if given[i] < reach]
        pool, remaining = sum([weights[i] for i in free]), rest
        for i in free:
            extra = min(reach - given[i], max(1, remaining * weights[i] // pool), rest)
            given[i] = given[i] + extra
            rest = rest - extra
    return np.array(given)


def noise(stream_key, dims, scale, reach, split=(), kind=jnp.bfloat16):
    values = scale * jax.random.normal(stream_key, dims, jnp.float32)
    if split:
        values = values * block_levels(stream_key, dims, split, -0.22, 0.18)
    return jnp.clip(values, -reach, reach).astype(kind)


def setup_inputs(seed: int = 0) -> dict:
    splits = jax.random.split(jax.random.key(seed), 12)
    tokens = noise(splits[0], (TOKENS, D), 1.0, 6.0, ((0, 4),))
    norm_gain = jnp.clip(1.0 + 0.18 * jax.random.normal(splits[1], (D,), jnp.float32), 0.1, 1.9)
    expert_ids_keys = jax.random.split(jax.random.fold_in(splits[2], 1), TOKENS // TOK_G)
    expert_ids_turns = jax.random.permutation(jax.random.fold_in(splits[2], 3), TOKENS // TOK_G)
    expert_ids = jax.vmap(lambda own, number: shared_out(jax.random.fold_in(splits[2], 2), own, number, TOK_G, EXPERTS, 2, CAP, 2))(expert_ids_keys, expert_ids_turns).reshape((TOKENS, 2))
    routing_weight = jnp.clip(0.1 + 0.9 * jax.random.uniform(splits[3], (TOKENS, 2), jnp.float32) ** block_levels(splits[3], (TOKENS, 2), ((0, 4),), -0.2, 0.2), 0.1, 1.0)
    expert_gate = noise(splits[4], (EXPERTS, D, FF), D ** -0.5, 0.125, ((0, 4), (2, 8)))
    expert_up = noise(splits[5], (EXPERTS, D, FF), D ** -0.5, 0.125, ((0, 4), (2, 8)))
    expert_down = noise(splits[6], (EXPERTS, FF, D), FF ** -0.5, 0.078125, ((0, 4), (1, 8)))
    dense_gate_w = noise(splits[7], (D, DS), D ** -0.5, 0.125, ((1, 8),))
    dense_up_w = noise(splits[8], (D, DS), D ** -0.5, 0.125, ((1, 8),))
    dense_down_w = noise(splits[9], (DS, D), DS ** -0.5, 0.1875, ((0, 8),))
    dense_gate = jnp.clip(jax.random.uniform(splits[10], (D,), jnp.float32, -3.0, 3.0) * block_levels(splits[10], (D,), ((0, 8),), -0.4, 0.0), -3.0, 3.0)
    return {"tokens": tokens, "norm_gain": norm_gain, "expert_ids": expert_ids, "routing_weight": routing_weight, "expert_gate": expert_gate, "expert_up": expert_up, "expert_down": expert_down, "dense_gate_w": dense_gate_w, "dense_up_w": dense_up_w, "dense_down_w": dense_down_w, "dense_gate": dense_gate}


EPSILON = 1e-06

def normalize(tokens, norm_gain):
    values = tokens.astype(jnp.float32)
    factor = lax.rsqrt(lax.optimization_barrier(jnp.mean(values * values, axis=-1, keepdims=True)) + EPSILON)
    return (values * factor * norm_gain[None, :]).astype(jnp.bfloat16)

def positions(block_ids):
    flat_ids = block_ids.reshape(-1)
    one_hot = (flat_ids[:, None] == jnp.arange(EXPERTS, dtype=jnp.int32)[None, :]).astype(jnp.int32)
    earlier = jnp.cumsum(one_hot, axis=0) - one_hot
    return flat_ids * CAP + lax.optimization_barrier(jnp.sum(earlier * one_hot, axis=1))

def fill_table(place_row):
    token_no = jnp.arange(2 * TOK_G, dtype=jnp.int32) // 2 + 1
    return jnp.zeros((EXPERTS * CAP,), jnp.int32).at[place_row].set(token_no)

def pick_rows(table, index_row):
    return table[index_row]

def block_sum(hidden, down_w, part_size):
    row_count = hidden.shape[0]
    pieces = hidden.reshape(row_count, N_TP, part_size).astype(jnp.float32)
    weights = down_w.reshape(N_TP, part_size, down_w.shape[1]).astype(jnp.float32)
    partial_value = jnp.einsum('rpf,pfd->rpd', pieces, weights).astype(jnp.bfloat16)
    partial_value = lax.optimization_barrier(partial_value)
    return lax.optimization_barrier(jnp.sum(partial_value.astype(jnp.float32), axis=1))

def reference(tokens, norm_gain, expert_ids, routing_weight, expert_gate, expert_up, expert_down, dense_gate_w, dense_up_w, dense_down_w, dense_gate):
    normed = normalize(tokens, norm_gain)
    normed_blocks = normed.reshape(N_EP, TOK_G, D)
    places = jax.vmap(positions)(expert_ids.reshape(N_EP, TOK_G, 2))
    sources = jax.vmap(fill_table)(places)
    padded = jnp.concatenate([jnp.zeros((N_EP, 1, D), jnp.bfloat16), normed_blocks], axis=1)
    gathered = jax.vmap(pick_rows)(padded, sources)
    expert_rows = gathered.reshape(N_EP, EXPERTS, CAP, D).transpose(1, 0, 2, 3).reshape(EXPERTS, N_EP * CAP, D)

    def one_expert(operands):
        rows_in, gate_w, up_w, down_w = operands
        gate_act = jnp.dot(rows_in, gate_w, preferred_element_type=jnp.float32)
        up_act = jnp.dot(rows_in, up_w, preferred_element_type=jnp.float32)
        hidden = (jax.nn.silu(gate_act) * up_act).astype(jnp.bfloat16)
        return block_sum(hidden, down_w, FF_PART)
    expert_out = lax.map(one_expert, (expert_rows, expert_gate, expert_up, expert_down)).astype(jnp.bfloat16)
    by_source = expert_out.reshape(EXPERTS, N_EP, CAP, D).transpose(1, 0, 2, 3).reshape(N_EP, EXPERTS * CAP, D)
    picked = jax.vmap(pick_rows)(by_source, places).reshape(TOKENS, 2, D).astype(jnp.float32)
    routed = lax.optimization_barrier(jnp.sum(routing_weight[:, :, None] * picked, axis=1))

    def dense_block(block_rows):
        gate_act = jnp.dot(block_rows, dense_gate_w, preferred_element_type=jnp.float32)
        up_act = jnp.dot(block_rows, dense_up_w, preferred_element_type=jnp.float32)
        hidden = (jax.nn.silu(gate_act) * up_act).astype(jnp.bfloat16)
        return block_sum(hidden, dense_down_w, DS_PART)
    dense_out = lax.map(dense_block, normed_blocks).reshape(TOKENS, D)
    layer_out = routed + jax.nn.sigmoid(dense_gate)[None, :] * dense_out
    return layer_out.astype(jnp.bfloat16)
```

```python
import jax
import jax.numpy as jnp
from jax import lax
from jax.experimental import pallas as pl
from jax.experimental.pallas import tpu as pltpu
from jax.sharding import PartitionSpec as P

EPSILON = 1e-06


def positions(block_ids, experts, capacity):
    flat_ids = block_ids.reshape(-1)
    one_hot = (flat_ids[:, None] == jnp.arange(experts, dtype=jnp.int32)[None, :]).astype(jnp.int32)
    earlier = jnp.cumsum(one_hot, axis=0) - one_hot
    return flat_ids * capacity + jnp.sum(earlier * one_hot, axis=1)


def transposed_term(hidden, down_w):
    return lax.dot_general(
        down_w, hidden, (((0,), (1,)), ((), ())), preferred_element_type=jnp.float32
    )


def plain_local(
    tokens,
    norm_gain,
    expert_ids,
    routing_weight,
    expert_gate,
    expert_up,
    expert_down,
    dense_gate_w,
    dense_up_w,
    dense_down_w,
    dense_gate,
):
    experts = lax.axis_size("ep")
    group_tokens, model_width = tokens.shape
    capacity = 3 * group_tokens // experts
    slots_all = experts * capacity
    part_rows = model_width // lax.axis_size("tp")
    values = tokens.astype(jnp.float32)
    factor = lax.rsqrt(jnp.mean(values * values, axis=-1, keepdims=True) + EPSILON)
    normed = (values * factor * norm_gain[None, :]).astype(jnp.bfloat16)
    places = positions(expert_ids, experts, capacity)
    token_no = jnp.arange(2 * group_tokens, dtype=jnp.int32) // 2 + 1
    sources = jnp.zeros((slots_all,), jnp.int32).at[places].set(token_no)
    padded = jnp.concatenate([jnp.zeros((1, model_width), jnp.bfloat16), normed], axis=0)
    gate_w = expert_gate[0]
    up_w = expert_up[0]
    down_w = expert_down[0]
    first_col = lax.axis_index("tp") * part_rows
    column_part = lax.dynamic_slice_in_dim(padded, first_col, part_rows, 1)
    outgoing = column_part[sources].reshape(experts, capacity, part_rows)
    landed = lax.all_to_all(outgoing, "ep", split_axis=0, concat_axis=0, tiled=True)
    portion = lax.all_gather(landed, "tp", axis=2, tiled=True)
    columns = portion.reshape(slots_all, portion.shape[2])
    gate_act = jnp.dot(columns, gate_w, preferred_element_type=jnp.float32)
    up_act = jnp.dot(columns, up_w, preferred_element_type=jnp.float32)
    hidden = (jax.nn.silu(gate_act) * up_act).astype(jnp.bfloat16)
    dense_gate_act = jnp.dot(normed, dense_gate_w, preferred_element_type=jnp.float32)
    dense_up_act = jnp.dot(normed, dense_up_w, preferred_element_type=jnp.float32)
    dense_hidden = (jax.nn.silu(dense_gate_act) * dense_up_act).astype(jnp.bfloat16)
    dense_out = lax.psum_scatter(
        transposed_term(dense_hidden, dense_down_w).astype(jnp.bfloat16),
        "tp",
        scatter_dimension=0,
        tiled=True,
    ).astype(jnp.float32)
    expert_out = lax.psum_scatter(
        transposed_term(hidden, down_w).astype(jnp.bfloat16), "tp", scatter_dimension=0, tiled=True
    )
    expert_half = expert_out.reshape(part_rows, experts, capacity)
    returned = lax.all_to_all(expert_half, "ep", split_axis=1, concat_axis=1, tiled=True).reshape(
        part_rows, slots_all
    )
    picked = (
        jnp.take(returned, places, axis=1).astype(jnp.float32).reshape(part_rows, group_tokens, 2)
    )
    routed = jnp.sum(picked * routing_weight[None, :, :], axis=2)
    gate_factor = jax.nn.sigmoid(dense_gate)[:, None]
    return (routed + gate_factor * dense_out).T.astype(jnp.bfloat16)


BF = jnp.bfloat16
F32 = jnp.float32


def silu_mul(gate_act, up_act):
    return (gate_act / (1.0 + jnp.exp(-gate_act)) * up_act).astype(BF)


def dot_t(rows, weights):
    return lax.dot_general(rows, weights, (((1,), (1,)), ((), ())), preferred_element_type=F32)


ORDER = (1, 2, 3)
SCHEDULE = (
    "N", "H00", "H01", "H02", "G10", "G11", "C1", "D", "P00", "P01", "G20", "G21", "C2",
    "X1", "Y1", "S1", "G30", "G31", "C3", "A0", "X2", "Y2", "S2", "L1", "H10", "H11",
    "H12", "P10", "X3", "Y3", "S3", "P11", "L2", "E0", "F0", "A1", "H20", "H21", "H22",
    "P20", "P21", "L3", "E1", "F1", "A2", "H30", "H31", "H32", "P30", "P31", "I1", "J1",
    "E2", "F2", "A3", "I0", "J0", "I2", "J2", "E3", "F3", "R1", "R2", "I3", "J3", "R3",
)


def fused_kernel(
    tok_ref,
    gain_ref,
    ids_ref,
    rw_ref,
    gw_hbm,
    uw_hbm,
    dw_hbm,
    dg_hbm,
    du_hbm,
    dd_hbm,
    dgate_ref,
    out_ref,
    gw,
    uw,
    dw,
    dgu,
    dd,
    factor,
    normed,
    slot_row,
    slot_col,
    weight_col,
    gates,
    zsend,
    xbuf,
    hid_l,
    hid_c,
    dhid,
    part_l,
    part_c,
    r0_l,
    r0_c,
    r1a_l,
    r1b_l,
    r1a_c,
    r1b_c,
    r2a_l,
    r2b_l,
    r2a_c,
    r2b_c,
    fin,
    ret,
    total,
    wsem,
    sems,
):
    me = lax.axis_index("ep")
    tp = lax.axis_index("tp")
    core, xx, yy = tp % 2, (tp // 2) % 2, tp // 4
    group, width = tok_ref.shape
    cols = out_ref.shape[1]
    rounds, cap = zsend.shape[:2]
    ffp = gw.shape[0]
    dsp = dd.shape[0]
    half = cap // 2
    mesh_id = pl.DeviceIdType.MESH
    to_core, to_x, to_y = 1, 2, 4

    def peer(flip):
        bits = (core + flip % 2) % 2, (xx + flip // 2 % 2) % 2, (yy + flip // 4) % 2
        return bits[2] * 4 + bits[1] * 2 + bits[0]

    def partner(j):
        return (me // 2 + j // 2) % 2 * 2 + (me % 2 + j % 2) % 2

    barrier = pltpu.get_barrier_semaphore()
    for flip in range(1, 8):
        pl.semaphore_signal(barrier, 1, device_id=(me, peer(flip)), device_id_type=mesh_id)
    for j in range(1, rounds + 1):
        pl.semaphore_signal(barrier, 1, device_id=(partner(j), tp), device_id_type=mesh_id)

    loads = {
        "g": pltpu.make_async_copy(gw_hbm.at[0], gw, wsem.at[0]),
        "u": pltpu.make_async_copy(uw_hbm.at[0], uw, wsem.at[1]),
        "dg": pltpu.make_async_copy(dg_hbm, dgu.at[:, pl.ds(0, dsp)], wsem.at[2]),
        "du": pltpu.make_async_copy(du_hbm, dgu.at[:, pl.ds(dsp, dsp)], wsem.at[3]),
        "d": pltpu.make_async_copy(dw_hbm.at[0], dw, wsem.at[4]),
        "dd": pltpu.make_async_copy(dd_hbm, dd, wsem.at[5]),
    }
    for load in loads.values():
        load.start()

    def need(*names):
        for name in names:
            if name in loads:
                loads.pop(name).wait()

    sent, arrived = {}, set()

    def send(name, src, dst, target):
        n = len(sent)
        copy = pltpu.make_async_remote_copy(
            src_ref=src,
            dst_ref=dst,
            send_sem=sems.at[0, n],
            recv_sem=sems.at[1, n],
            device_id=target,
            device_id_type=mesh_id,
        )
        copy.start()
        sent[name] = copy

    def got(*names):
        for name in names:
            if name not in arrived:
                sent[name].wait_recv()
                arrived.add(name)

    def at_tp(flip):
        return (me, peer(flip))

    def span(slice_no):
        return pl.ds(pl.multiple_of(slice_no * cols, cols), cols)

    step = 64
    for i in range(0, group, step):
        values = tok_ref[i : i + step, :].astype(F32)
        mean = jnp.sum(values * values, axis=1, keepdims=True) * (1.0 / width)
        factor[i : i + step, :] = jnp.broadcast_to(lax.rsqrt(mean + EPSILON), (step, 128))

    id0, id1 = ids_ref[0:1, :], ids_ref[1:2, :]
    number = lax.broadcasted_iota(jnp.int32, (128, group), 0)
    named = (id0 == number) | (id1 == number)
    earlier = jnp.where(
        lax.broadcasted_iota(jnp.int32, (group, group), 0)
        < lax.broadcasted_iota(jnp.int32, (group, group), 1),
        1.0,
        0.0,
    ).astype(BF)
    marks = jnp.where(named, 1.0, 0.0).astype(BF)
    count = jnp.dot(marks, earlier, preferred_element_type=F32)
    slots = jnp.where(named, count, -1.0)
    slot_row[...] = slots

    def pick(e):
        row = slot_row[pl.ds(e, 1), :].astype(jnp.int32)
        where = lax.broadcasted_iota(jnp.int32, (cap, group), 0)
        return jnp.where(row == where, 1.0, 0.0).astype(BF)

    own = (tok_ref[:, span(tp)].astype(F32) * factor[:, 0:1] * gain_ref[:, span(tp)]).astype(BF)
    tops = {0: pl.ds(0, half), 1: pl.ds(half, half)}
    gates[tp] = dgate_ref[...]
    for n, j in enumerate(ORDER):
        zsend[j - 1] = jnp.dot(pick(partner(j)), own, preferred_element_type=F32).astype(BF)
        if n == 0:
            pl.semaphore_wait(barrier, 7 + rounds)
        for h, rows in tops.items():
            send(("z", j, h), zsend.at[j - 1, rows], xbuf.at[j - 1, rows, span(tp)], (partner(j), tp))
    for flip in range(1, 8):
        send(("gate", flip), dgate_ref, gates.at[tp], at_tp(flip))

    weights = jnp.where(id0 == number, rw_ref[0:1, :], 0.0) + jnp.where(id1 == number, rw_ref[1:2, :], 0.0)
    slot_col[...] = slots.T
    weight_col[...] = weights.T
    lane = lax.broadcasted_iota(jnp.int32, (group, 128), 1)

    def weight_of(e):
        return jnp.sum(jnp.where(lane == e, weight_col[...], 0.0), axis=1, keepdims=True)

    def norm_all():
        gain = gain_ref[...]

        def body(i, carry):
            rows = pl.ds(pl.multiple_of(i * 32, 32), 32)
            values = tok_ref[rows, :].astype(F32)
            normed[rows, :] = (values * factor[rows, 0:1] * gain).astype(BF)
            return carry

        lax.fori_loop(0, group // 32, body, 0)

    def forward(name, j, rows, slice_flip, flip):
        ref = xbuf.at[j - 1, rows, span(peer(slice_flip))]
        send((name, j), ref, ref, at_tp(flip))

    everything = pl.ds(0, cap)

    def gather_start(j, h):
        got(("z", j, h))
        forward("x%d" % h, j, tops[h], 0, to_x)
        forward("y%d" % h, j, tops[h], 0, to_y)

    def gather_core(j):
        forward("c", j, everything, 0, to_core)

    def gather_relay_x(j):
        got(("x0", j))
        forward("xy", j, tops[0], to_x, to_y)

    def gather_relay_y(j):
        got(("y1", j))
        forward("yx", j, tops[1], to_y, to_x)

    def gather_share(j):
        got(("x0", j), ("x1", j))
        forward("xc", j, everything, to_x, to_core)
        got(("y0", j), ("y1", j))
        forward("yc", j, everything, to_y, to_core)

    def gather_last(j):
        got(("xy", j))
        forward("xyc", j, tops[0], to_x + to_y, to_core)
        got(("yx", j))
        forward("yxc", j, tops[1], to_x + to_y, to_core)

    tiles = [(n, min(256, ffp - n)) for n in range(0, ffp, 256)]

    def hidden_tile(b, t):
        need("g", "u")
        if b:
            got(*[(name, b) for name in ("c", "xc", "yc", "xyc", "yxc")])
        rows = xbuf[b - 1] if b else normed[...]
        n, size = tiles[t]
        value = silu_mul(dot_t(rows, gw[n : n + size, :]), dot_t(rows, uw[n : n + size, :]))
        if b:
            hid_c[b - 1, :, n : n + size] = value
        else:
            hid_l[:, n : n + size] = value

    def dense_hidden():
        need("dg", "du")
        acts = jnp.dot(normed[...], dgu[...], preferred_element_type=F32)
        dhid[...] = silu_mul(acts[:, :dsp], acts[:, dsp:])

    def rs_refs(b):
        if b == 0:
            return part_l, r0_l, r1a_l, r1b_l, r2a_l, r2b_l
        return tuple(r.at[b - 1] for r in (part_c, r0_c, r1a_c, r1b_c, r2a_c, r2b_c))

    def halves(b):
        h = (cap if b else group) // 2
        return pl.ds(0, h), pl.ds(h, h)

    def partial(b, mine):
        need("d", "dd")
        which = core if mine else 1 - core
        part, r0 = rs_refs(b)[:2]
        if b == 0:
            scale = weight_of(me)
            got(*[("gate", flip) for flip in range(1, 8)])
        for q in range(4):
            k = 2 * q + which
            if b:
                value = jnp.dot(hid_c[b - 1], dw[:, span(k)], preferred_element_type=F32)
            else:
                side = jnp.dot(dhid[...], dd[:, span(k)], preferred_element_type=F32)
                value = jnp.dot(hid_l[...], dw[:, span(k)], preferred_element_type=F32)
                value = scale * value + jax.nn.sigmoid(gates[k]) * side
            part[which, q // 2, q % 2] = value.astype(BF)
        if not mine:
            send(("r0", b), part.at[1 - core], r0, at_tp(to_core))

    def add(dst, index, other):
        dst[index] = (dst[index].astype(F32) + other.astype(F32)).astype(BF)

    def scatter_one(b):
        part, r0, r1a, r1b = rs_refs(b)[:4]
        top, bottom = halves(b)
        got(("r0", b))
        add(part, (core, 1 - yy, 1 - xx), r0[1 - yy, 1 - xx])
        send(("a0", b), part.at[core, 1 - yy, 1 - xx, top], r1a.at[1 - yy], at_tp(to_x))
        send(("b0", b), part.at[core, 1 - yy, 1 - xx, bottom], r1b.at[1 - xx], at_tp(to_y))
        add(part, (core, yy, 1 - xx), r0[yy, 1 - xx])
        send(("a1", b), part.at[core, yy, 1 - xx, top], r1a.at[yy], at_tp(to_x))
        add(part, (core, 1 - yy, xx), r0[1 - yy, xx])
        send(("b1", b), part.at[core, 1 - yy, xx, bottom], r1b.at[xx], at_tp(to_y))
        add(part, (core, yy, xx), r0[yy, xx])

    def scatter_two_a(b):
        part, r0, r1a, r1b, r2a, r2b = rs_refs(b)
        top, bottom = halves(b)
        got(("a0", b))
        add(part, (core, 1 - yy, xx, top), r1a[1 - yy])
        send(("a2", b), part.at[core, 1 - yy, xx, top], r2a, at_tp(to_y))

    def scatter_two_b(b):
        part, r0, r1a, r1b, r2a, r2b = rs_refs(b)
        top, bottom = halves(b)
        got(("b0", b))
        add(part, (core, yy, 1 - xx, bottom), r1b[1 - xx])
        send(("b2", b), part.at[core, yy, 1 - xx, bottom], r2b, at_tp(to_x))

    def finish(b, h, value):
        rows = halves(b)[h]
        if b == 0:
            total[rows, :] = value
        else:
            fin[b - 1, rows, :] = value.astype(BF)
            send(("ret", b, h), fin.at[b - 1, rows], ret.at[b - 1, rows], (partner(b), tp))

    def scatter_three_a(b):
        part, r0, r1a, r1b, r2a, r2b = rs_refs(b)
        got(("a1", b), ("a2", b))
        mine = part[core, yy, xx, halves(b)[0]].astype(F32)
        finish(b, 0, mine + r1a[yy].astype(F32) + r2a[...].astype(F32))

    def scatter_three_b(b):
        part, r0, r1a, r1b, r2a, r2b = rs_refs(b)
        got(("b1", b), ("b2", b))
        mine = part[core, yy, xx, halves(b)[1]].astype(F32)
        finish(b, 1, mine + r1b[xx].astype(F32) + r2b[...].astype(F32))

    def returned(j):
        e = partner(j)
        slot = jnp.sum(jnp.where(lane == e, slot_col[...], 0.0), axis=1, keepdims=True).astype(jnp.int32)
        place = jnp.where(slot == lax.broadcasted_iota(jnp.int32, (group, cap), 1), 1.0, 0.0).astype(BF)
        scale = weight_of(e)
        got(("ret", j, 0), ("ret", j, 1))
        total[...] += scale * jnp.dot(place, ret[j - 1], preferred_element_type=F32)

    steps = {
        "N": norm_all,
        "G": gather_start,
        "C": gather_core,
        "X": gather_relay_x,
        "Y": gather_relay_y,
        "S": gather_share,
        "L": gather_last,
        "H": hidden_tile,
        "D": dense_hidden,
        "P": partial,
        "A": scatter_one,
        "E": scatter_two_a,
        "F": scatter_two_b,
        "I": scatter_three_a,
        "J": scatter_three_b,
        "R": returned,
    }
    for word in SCHEDULE:
        steps[word[0]](*[int(digit) for digit in word[1:]])
    out_ref[...] = total[...].astype(BF)
    for copy in sent.values():
        copy.wait_send()


def fused_local(
    tokens,
    norm_gain,
    expert_ids,
    routing_weight,
    expert_gate,
    expert_up,
    expert_down,
    dense_gate_w,
    dense_up_w,
    dense_down_w,
    dense_gate,
):
    experts = lax.axis_size("ep")
    parts = lax.axis_size("tp")
    group, width = tokens.shape
    cap = 3 * group // experts
    cols = width // parts
    ffp = expert_gate.shape[2]
    dsp = dense_gate_w.shape[1]
    rounds = experts - 1
    vmem, hbm = pl.BlockSpec(memory_space=pltpu.VMEM), pl.BlockSpec(memory_space=pl.ANY)
    dma = pltpu.SemaphoreType.DMA
    half, ghalf = cap // 2, group // 2
    return pl.pallas_call(
        fused_kernel,
        out_shape=jax.ShapeDtypeStruct((group, cols), BF),
        in_specs=[vmem] * 4 + [hbm] * 6 + [vmem],
        out_specs=vmem,
        scratch_shapes=[
            pltpu.VMEM((ffp, width), BF),
            pltpu.VMEM((ffp, width), BF),
            pltpu.VMEM((ffp, width), BF),
            pltpu.VMEM((width, 2 * dsp), BF),
            pltpu.VMEM((dsp, width), BF),
            pltpu.VMEM((group, 128), F32),
            pltpu.VMEM((group, width), BF),
            pltpu.VMEM((128, group), F32),
            pltpu.VMEM((group, 128), F32),
            pltpu.VMEM((group, 128), F32),
            pltpu.VMEM((parts, 1, cols), F32),
            pltpu.VMEM((rounds, cap, cols), BF),
            pltpu.VMEM((rounds, cap, width), BF),
            pltpu.VMEM((group, ffp), BF),
            pltpu.VMEM((rounds, cap, ffp), BF),
            pltpu.VMEM((group, dsp), BF),
            pltpu.VMEM((2, 2, 2, group, cols), BF),
            pltpu.VMEM((rounds, 2, 2, 2, cap, cols), BF),
            pltpu.VMEM((2, 2, group, cols), BF),
            pltpu.VMEM((rounds, 2, 2, cap, cols), BF),
            pltpu.VMEM((2, ghalf, cols), BF),
            pltpu.VMEM((2, ghalf, cols), BF),
            pltpu.VMEM((rounds, 2, half, cols), BF),
            pltpu.VMEM((rounds, 2, half, cols), BF),
            pltpu.VMEM((ghalf, cols), BF),
            pltpu.VMEM((ghalf, cols), BF),
            pltpu.VMEM((rounds, half, cols), BF),
            pltpu.VMEM((rounds, half, cols), BF),
            pltpu.VMEM((rounds, cap, cols), BF),
            pltpu.VMEM((rounds, cap, cols), BF),
            pltpu.VMEM((group, cols), F32),
            dma((6,)),
            dma((2, 84)),
        ],
        compiler_params=pltpu.CompilerParams(
            collective_id=0, has_side_effects=True, vmem_limit_bytes=56 * 1024 * 1024
        ),
        name="routed_layer",
    )(
        tokens,
        norm_gain[None, :],
        expert_ids.T,
        routing_weight.T,
        jnp.swapaxes(expert_gate, 1, 2),
        jnp.swapaxes(expert_up, 1, 2),
        expert_down,
        dense_gate_w,
        dense_up_w,
        dense_down_w,
        dense_gate[None, :],
    )


def local(*args):
    experts, parts = lax.axis_size("ep"), lax.axis_size("tp")
    group, width = args[0].shape
    fits = (
        experts == 4
        and parts == 8
        and width % (128 * parts) == 0
        and group % 128 == 0
        and (3 * group // experts) % 32 == 0
        and args[7].shape[1] % 128 == 0
        and args[4].shape[2] % 16 == 0
    )
    return (fused_local if fits else plain_local)(*args)


def solution(mesh):
    return jax.shard_map(
        local,
        mesh=mesh,
        in_specs=(
            P("ep", None),
            P(),
            P("ep", None),
            P("ep", None),
            P("ep", None, "tp"),
            P("ep", None, "tp"),
            P("ep", "tp", None),
            P(None, "tp"),
            P(None, "tp"),
            P("tp", None),
            P("tp"),
        ),
        out_specs=P("ep", "tp"),
        check_vma=False,
    )
```

```python
import jax
import jax.numpy as jnp
from jax import lax
from jax.experimental import pallas as pl
from jax.experimental.pallas import tpu as pltpu
from jax.sharding import PartitionSpec as P

EPSILON = 1e-06


def positions(block_ids, experts, capacity):
    flat_ids = block_ids.reshape(-1)
    one_hot = (flat_ids[:, None] == jnp.arange(experts, dtype=jnp.int32)[None, :]).astype(jnp.int32)
    earlier = jnp.cumsum(one_hot, axis=0) - one_hot
    return flat_ids * capacity + jnp.sum(earlier * one_hot, axis=1)


def transposed_term(hidden, down_w):
    return lax.dot_general(
        down_w, hidden, (((0,), (1,)), ((), ())), preferred_element_type=jnp.float32
    )


def plain_local(
    tokens,
    norm_gain,
    expert_ids,
    routing_weight,
    expert_gate,
    expert_up,
    expert_down,
    dense_gate_w,
    dense_up_w,
    dense_down_w,
    dense_gate,
):
    experts = lax.axis_size("ep")
    group_tokens, model_width = tokens.shape
    capacity = 3 * group_tokens // experts
    slots_all = experts * capacity
    part_rows = model_width // lax.axis_size("tp")
    values = tokens.astype(jnp.float32)
    factor = lax.rsqrt(jnp.mean(values * values, axis=-1, keepdims=True) + EPSILON)
    normed = (values * factor * norm_gain[None, :]).astype(jnp.bfloat16)
    places = positions(expert_ids, experts, capacity)
    token_no = jnp.arange(2 * group_tokens, dtype=jnp.int32) // 2 + 1
    sources = jnp.zeros((slots_all,), jnp.int32).at[places].set(token_no)
    padded = jnp.concatenate([jnp.zeros((1, model_width), jnp.bfloat16), normed], axis=0)
    gate_w = expert_gate[0]
    up_w = expert_up[0]
    down_w = expert_down[0]
    first_col = lax.axis_index("tp") * part_rows
    column_part = lax.dynamic_slice_in_dim(padded, first_col, part_rows, 1)
    outgoing = column_part[sources].reshape(experts, capacity, part_rows)
    landed = lax.all_to_all(outgoing, "ep", split_axis=0, concat_axis=0, tiled=True)
    portion = lax.all_gather(landed, "tp", axis=2, tiled=True)
    columns = portion.reshape(slots_all, portion.shape[2])
    gate_act = jnp.dot(columns, gate_w, preferred_element_type=jnp.float32)
    up_act = jnp.dot(columns, up_w, preferred_element_type=jnp.float32)
    hidden = (jax.nn.silu(gate_act) * up_act).astype(jnp.bfloat16)
    dense_gate_act = jnp.dot(normed, dense_gate_w, preferred_element_type=jnp.float32)
    dense_up_act = jnp.dot(normed, dense_up_w, preferred_element_type=jnp.float32)
    dense_hidden = (jax.nn.silu(dense_gate_act) * dense_up_act).astype(jnp.bfloat16)
    dense_out = lax.psum_scatter(
        transposed_term(dense_hidden, dense_down_w).astype(jnp.bfloat16),
        "tp",
        scatter_dimension=0,
        tiled=True,
    ).astype(jnp.float32)
    expert_out = lax.psum_scatter(
        transposed_term(hidden, down_w).astype(jnp.bfloat16), "tp", scatter_dimension=0, tiled=True
    )
    expert_half = expert_out.reshape(part_rows, experts, capacity)
    returned = lax.all_to_all(expert_half, "ep", split_axis=1, concat_axis=1, tiled=True).reshape(
        part_rows, slots_all
    )
    picked = (
        jnp.take(returned, places, axis=1).astype(jnp.float32).reshape(part_rows, group_tokens, 2)
    )
    routed = jnp.sum(picked * routing_weight[None, :, :], axis=2)
    gate_factor = jax.nn.sigmoid(dense_gate)[:, None]
    return (routed + gate_factor * dense_out).T.astype(jnp.bfloat16)


BF = jnp.bfloat16
F32 = jnp.float32


def silu_mul(gate_act, up_act):
    return (gate_act / (1.0 + jnp.exp(-gate_act)) * up_act).astype(BF)


def dot_t(rows, weights):
    return lax.dot_general(rows, weights, (((1,), (1,)), ((), ())), preferred_element_type=F32)


SOURCES = ((3, 2, 1), (0, 3, 2), (3, 0, 1), (0, 1, 2))
TARGETS = ((3, 1, 2), (0, 3, 2), (3, 0, 1), (0, 2, 1))
SCHEDULE = (
    "N", "G10", "H01", "G11", "D", "G20", "H00", "G21", "H02", "Y1", "C1", "X1", "G31",
    "S1", "G30", "X2", "C2", "P00", "Y2", "L1", "P01", "A00", "C3", "H12", "Y3", "H10",
    "S2", "X3", "H11", "L2", "A01", "S3", "P10", "P11", "H22", "A10", "H21", "A11",
    "F0", "L3", "H20", "E0", "P20", "H30", "E1", "P21", "A20", "H32", "A21", "H31",
    "P30", "F1", "P31", "J0", "I1", "E2", "A30", "F2", "A31", "J1", "I0", "E3", "I2",
    "F3", "J2", "I3", "J3", "R1", "R2", "R3",
)


def fused_kernel(
    tok_ref,
    gain_ref,
    ids_ref,
    rw_ref,
    gw_hbm,
    uw_hbm,
    dw_hbm,
    dg_hbm,
    du_hbm,
    dd_hbm,
    dgate_ref,
    out_ref,
    gw,
    uw,
    dw,
    dgu,
    dd,
    factor,
    normed,
    slot_row,
    slot_col,
    weight_col,
    gates,
    zsend,
    xbuf,
    hid_l,
    hid_c,
    dhid,
    part_l,
    part_c,
    r0_l,
    r0_c,
    r1a_l,
    r1b_l,
    r1a_c,
    r1b_c,
    r2a_l,
    r2b_l,
    r2a_c,
    r2b_c,
    fin,
    ret,
    total,
    wsem,
    zsem,
    rsem,
    sems,
):
    me = lax.axis_index("ep")
    tp = lax.axis_index("tp")
    core, xx, yy = tp % 2, (tp // 2) % 2, tp // 4
    group, width = tok_ref.shape
    cols = out_ref.shape[1]
    rounds, cap = zsend.shape[:2]
    ffp = gw.shape[0]
    dsp = dd.shape[0]
    half = cap // 2
    mesh_id = pl.DeviceIdType.MESH
    to_core, to_x, to_y = 1, 2, 4

    def peer(flip):
        bits = (core + flip % 2) % 2, (xx + flip // 2 % 2) % 2, (yy + flip // 4) % 2
        return bits[2] * 4 + bits[1] * 2 + bits[0]

    place_value = (1 + 3 * (me % 2)) * (1 + 15 * (me // 2))

    def lookup(row):
        return sum(value * 4**plane for plane, value in enumerate(row)) // place_value % 4

    def source(slot):
        return lookup([row[slot - 1] for row in SOURCES])

    def slot_at(other):
        return lookup([SOURCES[q].index(p) for p, q in enumerate(other)])

    barrier = pltpu.get_barrier_semaphore()
    for flip in range(1, 8):
        pl.semaphore_signal(barrier, 1, device_id=(me, peer(flip)), device_id_type=mesh_id)
    for j in range(1, rounds + 1):
        pl.semaphore_signal(
            barrier, 1, device_id=((me + j) % 4, peer(to_core)), device_id_type=mesh_id
        )

    loads = {
        "g": pltpu.make_async_copy(gw_hbm.at[0], gw, wsem.at[0]),
        "u": pltpu.make_async_copy(uw_hbm.at[0], uw, wsem.at[1]),
        "dg": pltpu.make_async_copy(dg_hbm, dgu.at[:, pl.ds(0, dsp)], wsem.at[2]),
        "du": pltpu.make_async_copy(du_hbm, dgu.at[:, pl.ds(dsp, dsp)], wsem.at[3]),
        "d": pltpu.make_async_copy(dw_hbm.at[0], dw, wsem.at[4]),
        "dd": pltpu.make_async_copy(dd_hbm, dd, wsem.at[5]),
    }
    for load in loads.values():
        load.start()

    def need(*names):
        for name in names:
            if name in loads:
                loads.pop(name).wait()

    started, expected = [], {}

    def transfer(src, dst, send_sem, recv_sem, target):
        return pltpu.make_async_remote_copy(
            src_ref=src,
            dst_ref=dst,
            send_sem=send_sem,
            recv_sem=recv_sem,
            device_id=target,
            device_id_type=mesh_id,
        )

    def send(name, src, dst, target):
        n = len(started)
        copy = transfer(src, dst, sems.at[0, n], sems.at[1, n], target)
        copy.start()
        started.append(copy)
        expected[name] = copy

    def got(*names):
        for name in names:
            if expected[name] is not None:
                expected[name].wait_recv()
                expected[name] = None

    def hop(sem, src, dst, number, landing, h, plane):
        rows = tops[h]
        copy = transfer(
            src.at[number, rows],
            dst(landing, rows, tp),
            sem.at[0, number, h],
            sem.at[1, landing, h],
            (plane, peer(to_core)),
        )
        copy.start()
        started.append(copy)

    def z_place(slot, rows, part):
        return xbuf.at[slot, rows, span(part)]

    def r_place(slot, rows, part):
        return ret.at[slot, rows]

    def at_tp(flip):
        return (me, peer(flip))

    tops = {0: pl.ds(0, half), 1: pl.ds(half, half)}

    def span(slice_no):
        return pl.ds(pl.multiple_of(slice_no * cols, cols), cols)

    step = 64
    for i in range(0, group, step):
        values = tok_ref[i : i + step, :].astype(F32)
        mean = jnp.sum(values * values, axis=1, keepdims=True) * (1.0 / width)
        factor[i : i + step, :] = jnp.broadcast_to(lax.rsqrt(mean + EPSILON), (step, 128))

    id0, id1 = ids_ref[0:1, :], ids_ref[1:2, :]
    number = lax.broadcasted_iota(jnp.int32, (128, group), 0)
    named = (id0 == number) | (id1 == number)
    earlier = jnp.where(
        lax.broadcasted_iota(jnp.int32, (group, group), 0)
        < lax.broadcasted_iota(jnp.int32, (group, group), 1),
        1.0,
        0.0,
    ).astype(BF)
    marks = jnp.where(named, 1.0, 0.0).astype(BF)
    count = jnp.dot(marks, earlier, preferred_element_type=F32)
    slots = jnp.where(named, count, -1.0)
    slot_row[...] = slots

    def pick(e):
        row = slot_row[pl.ds(e, 1), :].astype(jnp.int32)
        where = lax.broadcasted_iota(jnp.int32, (cap, group), 0)
        return jnp.where(row == where, 1.0, 0.0).astype(BF)

    own = (tok_ref[:, span(tp)].astype(F32) * factor[:, 0:1] * gain_ref[:, span(tp)]).astype(BF)
    gates[tp] = dgate_ref[...]
    for n in range(rounds):
        targets = [row[n] for row in TARGETS]
        plane = lookup(targets)
        zsend[n] = jnp.dot(pick(plane), own, preferred_element_type=F32).astype(BF)
        if n == 0:
            pl.semaphore_wait(barrier, 7 + rounds)
        for h in tops:
            hop(zsem, zsend, z_place, n, slot_at(targets), h, plane)
    for n in range(rounds):
        for h, rows in tops.items():
            for kind, sem, src, place in (("z", zsem, zsend, z_place), ("r", rsem, fin, r_place)):
                landed = place(n, rows, peer(to_core))
                expected[kind, n + 1, h] = transfer(
                    src.at[n, rows], landed, sem.at[0, n, h], sem.at[1, n, h], at_tp(to_core)
                )
    for flip in range(1, 8):
        send(("gate", flip), dgate_ref, gates.at[tp], at_tp(flip))

    weights = jnp.where(id0 == number, rw_ref[0:1, :], 0.0) + jnp.where(id1 == number, rw_ref[1:2, :], 0.0)
    slot_col[...] = slots.T
    weight_col[...] = weights.T
    lane = lax.broadcasted_iota(jnp.int32, (group, 128), 1)

    def weight_of(e):
        return jnp.sum(jnp.where(lane == e, weight_col[...], 0.0), axis=1, keepdims=True)

    def norm_all():
        gain = gain_ref[...]

        def body(i, carry):
            rows = pl.ds(pl.multiple_of(i * 32, 32), 32)
            values = tok_ref[rows, :].astype(F32)
            normed[rows, :] = (values * factor[rows, 0:1] * gain).astype(BF)
            return carry

        lax.fori_loop(0, group // 32, body, 0)

    def forward(name, j, rows, slice_flip, flip):
        ref = xbuf.at[j - 1, rows, span(peer(slice_flip))]
        send((name, j), ref, ref, at_tp(flip))

    everything = pl.ds(0, cap)

    def gather_start(j, h):
        got(("z", j, h))
        forward("x%d" % h, j, tops[h], to_core, to_x + to_core)
        forward("y%d" % h, j, tops[h], to_core, to_y + to_core)

    def gather_core(j):
        forward("c", j, everything, to_core, to_core)

    def gather_relay_x(j):
        got(("x0", j))
        forward("xy", j, tops[0], to_x, to_y + to_core)

    def gather_relay_y(j):
        got(("y1", j))
        forward("yx", j, tops[1], to_y, to_x + to_core)

    def gather_share(j):
        got(("x0", j), ("x1", j))
        forward("xc", j, everything, to_x, to_core)
        got(("y0", j), ("y1", j))
        forward("yc", j, everything, to_y, to_core)

    def gather_last(j):
        got(("xy", j))
        forward("xyc", j, tops[0], 7, to_core)
        got(("yx", j))
        forward("yxc", j, tops[1], 7, to_core)

    tiles = [(n, min(256, ffp - n)) for n in range(0, ffp, 256)]

    def hidden_tile(b, t):
        need("g", "u")
        if b:
            got(*[(name, b) for name in ("c", "xc", "yc", "xyc", "yxc")])
        rows = xbuf[b - 1] if b else normed[...]
        n, size = tiles[t]
        value = silu_mul(dot_t(rows, gw[n : n + size, :]), dot_t(rows, uw[n : n + size, :]))
        if b:
            hid_c[b - 1, :, n : n + size] = value
        else:
            hid_l[:, n : n + size] = value

    def dense_hidden():
        need("dg", "du")
        acts = jnp.dot(normed[...], dgu[...], preferred_element_type=F32)
        dhid[...] = silu_mul(acts[:, :dsp], acts[:, dsp:])

    def rs_refs(b):
        if b == 0:
            return part_l, r0_l, r1a_l, r1b_l, r2a_l, r2b_l
        return tuple(r.at[b - 1] for r in (part_c, r0_c, r1a_c, r1b_c, r2a_c, r2b_c))

    def halves(b):
        h = (cap if b else group) // 2
        return pl.ds(0, h), pl.ds(h, h)

    def partial(b, mine):
        need("d", "dd")
        half_no = 0 if mine else 1
        swap = half_no + (1 if b else 0)
        part, r0 = rs_refs(b)[:2]
        if b == 0:
            scale = weight_of(me)
            got(*[("gate", flip) for flip in range(1, 8)])
        corners = ((1 - yy, 1 - xx), (yy, 1 - xx), (1 - yy, xx), (yy, xx))
        for (y, x), odd in zip(corners, (0, 1, 1, 0)):
            k = 4 * y + 2 * x + (core + odd + swap) % 2
            if b:
                value = jnp.dot(hid_c[b - 1], dw[:, span(k)], preferred_element_type=F32)
            else:
                side = jnp.dot(dhid[...], dd[:, span(k)], preferred_element_type=F32)
                value = jnp.dot(hid_l[...], dw[:, span(k)], preferred_element_type=F32)
                value = scale * value + jax.nn.sigmoid(gates[k]) * side
            part[half_no, y, x] = value.astype(BF)
        if not mine:
            for q, (y, x) in enumerate(corners):
                send(("r0", q, b), part.at[half_no, y, x], r0.at[y, x], at_tp(to_core))

    def add(dst, index, other):
        dst[index] = (dst[index].astype(F32) + other.astype(F32)).astype(BF)

    def scatter_one(b, late):
        part, r0, r1a, r1b = rs_refs(b)[:4]
        top, bottom = halves(b)
        if not late:
            got(("r0", 0, b))
            add(part, (0, 1 - yy, 1 - xx), r0[1 - yy, 1 - xx])
            send(("a0", b), part.at[0, 1 - yy, 1 - xx, top], r1a.at[1 - yy], at_tp(to_x + to_core))
            send(("b0", b), part.at[0, 1 - yy, 1 - xx, bottom], r1b.at[1 - xx], at_tp(to_y + to_core))
        else:
            got(("r0", 1, b))
            add(part, (0, yy, 1 - xx), r0[yy, 1 - xx])
            send(("a1", b), part.at[0, yy, 1 - xx, top], r1a.at[yy], at_tp(to_x + to_core))
            got(("r0", 2, b))
            add(part, (0, 1 - yy, xx), r0[1 - yy, xx])
            send(("b1", b), part.at[0, 1 - yy, xx, bottom], r1b.at[xx], at_tp(to_y + to_core))

    def scatter_two_a(b):
        part, r0, r1a, r1b, r2a, r2b = rs_refs(b)
        top, bottom = halves(b)
        got(("a0", b))
        add(part, (0, 1 - yy, xx, top), r1a[1 - yy])
        send(("a2", b), part.at[0, 1 - yy, xx, top], r2a, at_tp(to_y + to_core))

    def scatter_two_b(b):
        part, r0, r1a, r1b, r2a, r2b = rs_refs(b)
        top, bottom = halves(b)
        got(("b0", b))
        add(part, (0, yy, 1 - xx, bottom), r1b[1 - xx])
        send(("b2", b), part.at[0, yy, 1 - xx, bottom], r2b, at_tp(to_x + to_core))

    def finish(b, h, value):
        rows = halves(b)[h]
        if b == 0:
            total[rows, :] = value
        else:
            fin[b - 1, rows, :] = value.astype(BF)
            sources = [row[b - 1] for row in SOURCES]
            hop(rsem, fin, r_place, b - 1, slot_at(sources), h, source(b))

    def scatter_three_a(b):
        part, r0, r1a, r1b, r2a, r2b = rs_refs(b)
        rows = halves(b)[0]
        got(("r0", 3, b), ("a1", b), ("a2", b))
        mine = part[0, yy, xx, rows].astype(F32) + r0[yy, xx, rows].astype(F32)
        finish(b, 0, mine + r1a[yy].astype(F32) + r2a[...].astype(F32))

    def scatter_three_b(b):
        part, r0, r1a, r1b, r2a, r2b = rs_refs(b)
        rows = halves(b)[1]
        got(("r0", 3, b), ("b1", b), ("b2", b))
        mine = part[0, yy, xx, rows].astype(F32) + r0[yy, xx, rows].astype(F32)
        finish(b, 1, mine + r1b[xx].astype(F32) + r2b[...].astype(F32))

    def returned(j):
        e = source(j)
        slot = jnp.sum(jnp.where(lane == e, slot_col[...], 0.0), axis=1, keepdims=True).astype(jnp.int32)
        place = jnp.where(slot == lax.broadcasted_iota(jnp.int32, (group, cap), 1), 1.0, 0.0).astype(BF)
        scale = weight_of(e)
        got(("r", j, 0), ("r", j, 1))
        total[...] += scale * jnp.dot(place, ret[j - 1], preferred_element_type=F32)

    steps = {
        "N": norm_all,
        "G": gather_start,
        "C": gather_core,
        "X": gather_relay_x,
        "Y": gather_relay_y,
        "S": gather_share,
        "L": gather_last,
        "H": hidden_tile,
        "D": dense_hidden,
        "P": partial,
        "A": scatter_one,
        "E": scatter_two_a,
        "F": scatter_two_b,
        "I": scatter_three_a,
        "J": scatter_three_b,
        "R": returned,
    }
    for word in SCHEDULE:
        steps[word[0]](*[int(digit) for digit in word[1:]])
    out_ref[...] = total[...].astype(BF)
    for copy in started:
        copy.wait_send()


def fused_local(
    tokens,
    norm_gain,
    expert_ids,
    routing_weight,
    expert_gate,
    expert_up,
    expert_down,
    dense_gate_w,
    dense_up_w,
    dense_down_w,
    dense_gate,
):
    experts = lax.axis_size("ep")
    parts = lax.axis_size("tp")
    group, width = tokens.shape
    cap = 3 * group // experts
    cols = width // parts
    ffp = expert_gate.shape[2]
    dsp = dense_gate_w.shape[1]
    rounds = experts - 1
    vmem, hbm = pl.BlockSpec(memory_space=pltpu.VMEM), pl.BlockSpec(memory_space=pl.ANY)
    dma = pltpu.SemaphoreType.DMA
    half, ghalf = cap // 2, group // 2
    return pl.pallas_call(
        fused_kernel,
        out_shape=jax.ShapeDtypeStruct((group, cols), BF),
        in_specs=[vmem] * 4 + [hbm] * 6 + [vmem],
        out_specs=vmem,
        scratch_shapes=[
            pltpu.VMEM((ffp, width), BF),
            pltpu.VMEM((ffp, width), BF),
            pltpu.VMEM((ffp, width), BF),
            pltpu.VMEM((width, 2 * dsp), BF),
            pltpu.VMEM((dsp, width), BF),
            pltpu.VMEM((group, 128), F32),
            pltpu.VMEM((group, width), BF),
            pltpu.VMEM((128, group), F32),
            pltpu.VMEM((group, 128), F32),
            pltpu.VMEM((group, 128), F32),
            pltpu.VMEM((parts, 1, cols), F32),
            pltpu.VMEM((rounds, cap, cols), BF),
            pltpu.VMEM((rounds, cap, width), BF),
            pltpu.VMEM((group, ffp), BF),
            pltpu.VMEM((rounds, cap, ffp), BF),
            pltpu.VMEM((group, dsp), BF),
            pltpu.VMEM((2, 2, 2, group, cols), BF),
            pltpu.VMEM((rounds, 2, 2, 2, cap, cols), BF),
            pltpu.VMEM((2, 2, group, cols), BF),
            pltpu.VMEM((rounds, 2, 2, cap, cols), BF),
            pltpu.VMEM((2, ghalf, cols), BF),
            pltpu.VMEM((2, ghalf, cols), BF),
            pltpu.VMEM((rounds, 2, half, cols), BF),
            pltpu.VMEM((rounds, 2, half, cols), BF),
            pltpu.VMEM((ghalf, cols), BF),
            pltpu.VMEM((ghalf, cols), BF),
            pltpu.VMEM((rounds, half, cols), BF),
            pltpu.VMEM((rounds, half, cols), BF),
            pltpu.VMEM((rounds, cap, cols), BF),
            pltpu.VMEM((rounds, cap, cols), BF),
            pltpu.VMEM((group, cols), F32),
            dma((6,)),
            dma((2, rounds, 2)),
            dma((2, rounds, 2)),
            dma((2, 92)),
        ],
        compiler_params=pltpu.CompilerParams(
            collective_id=0, has_side_effects=True, vmem_limit_bytes=56 * 1024 * 1024
        ),
        name="routed_layer",
    )(
        tokens,
        norm_gain[None, :],
        expert_ids.T,
        routing_weight.T,
        jnp.swapaxes(expert_gate, 1, 2),
        jnp.swapaxes(expert_up, 1, 2),
        expert_down,
        dense_gate_w,
        dense_up_w,
        dense_down_w,
        dense_gate[None, :],
    )


def local(*args):
    experts, parts = lax.axis_size("ep"), lax.axis_size("tp")
    group, width = args[0].shape
    fits = (
        experts == 4
        and parts == 8
        and width % (128 * parts) == 0
        and group % 128 == 0
        and (3 * group // experts) % 32 == 0
        and args[7].shape[1] % 128 == 0
        and args[4].shape[2] % 16 == 0
    )
    return (fused_local if fits else plain_local)(*args)


def solution(mesh):
    return jax.shard_map(
        local,
        mesh=mesh,
        in_specs=(
            P("ep", None),
            P(),
            P("ep", None),
            P("ep", None),
            P("ep", None, "tp"),
            P("ep", None, "tp"),
            P("ep", "tp", None),
            P(None, "tp"),
            P(None, "tp"),
            P("tp", None),
            P("tp"),
        ),
        out_specs=P("ep", "tp"),
        check_vma=False,
    )
```

```python
import jax
import jax.numpy as jnp
from jax import lax
from jax.experimental import pallas as pl
from jax.experimental.pallas import tpu as pltpu
from jax.sharding import PartitionSpec as P

EPSILON = 1e-06


def positions(block_ids, experts, capacity):
    flat_ids = block_ids.reshape(-1)
    one_hot = (flat_ids[:, None] == jnp.arange(experts, dtype=jnp.int32)[None, :]).astype(jnp.int32)
    earlier = jnp.cumsum(one_hot, axis=0) - one_hot
    return flat_ids * capacity + jnp.sum(earlier * one_hot, axis=1)


def transposed_term(hidden, down_w):
    return lax.dot_general(
        down_w, hidden, (((0,), (1,)), ((), ())), preferred_element_type=jnp.float32
    )


def plain_local(
    tokens,
    norm_gain,
    expert_ids,
    routing_weight,
    expert_gate,
    expert_up,
    expert_down,
    dense_gate_w,
    dense_up_w,
    dense_down_w,
    dense_gate,
):
    experts = lax.axis_size("ep")
    group_tokens, model_width = tokens.shape
    capacity = 3 * group_tokens // experts
    slots_all = experts * capacity
    part_rows = model_width // lax.axis_size("tp")
    values = tokens.astype(jnp.float32)
    factor = lax.rsqrt(jnp.mean(values * values, axis=-1, keepdims=True) + EPSILON)
    normed = (values * factor * norm_gain[None, :]).astype(jnp.bfloat16)
    places = positions(expert_ids, experts, capacity)
    token_no = jnp.arange(2 * group_tokens, dtype=jnp.int32) // 2 + 1
    sources = jnp.zeros((slots_all,), jnp.int32).at[places].set(token_no)
    padded = jnp.concatenate([jnp.zeros((1, model_width), jnp.bfloat16), normed], axis=0)
    gate_w = expert_gate[0]
    up_w = expert_up[0]
    down_w = expert_down[0]
    first_col = lax.axis_index("tp") * part_rows
    column_part = lax.dynamic_slice_in_dim(padded, first_col, part_rows, 1)
    outgoing = column_part[sources].reshape(experts, capacity, part_rows)
    landed = lax.all_to_all(outgoing, "ep", split_axis=0, concat_axis=0, tiled=True)
    portion = lax.all_gather(landed, "tp", axis=2, tiled=True)
    columns = portion.reshape(slots_all, portion.shape[2])
    gate_act = jnp.dot(columns, gate_w, preferred_element_type=jnp.float32)
    up_act = jnp.dot(columns, up_w, preferred_element_type=jnp.float32)
    hidden = (jax.nn.silu(gate_act) * up_act).astype(jnp.bfloat16)
    dense_gate_act = jnp.dot(normed, dense_gate_w, preferred_element_type=jnp.float32)
    dense_up_act = jnp.dot(normed, dense_up_w, preferred_element_type=jnp.float32)
    dense_hidden = (jax.nn.silu(dense_gate_act) * dense_up_act).astype(jnp.bfloat16)
    dense_out = lax.psum_scatter(
        transposed_term(dense_hidden, dense_down_w).astype(jnp.bfloat16),
        "tp",
        scatter_dimension=0,
        tiled=True,
    ).astype(jnp.float32)
    expert_out = lax.psum_scatter(
        transposed_term(hidden, down_w).astype(jnp.bfloat16), "tp", scatter_dimension=0, tiled=True
    )
    expert_half = expert_out.reshape(part_rows, experts, capacity)
    returned = lax.all_to_all(expert_half, "ep", split_axis=1, concat_axis=1, tiled=True).reshape(
        part_rows, slots_all
    )
    picked = (
        jnp.take(returned, places, axis=1).astype(jnp.float32).reshape(part_rows, group_tokens, 2)
    )
    routed = jnp.sum(picked * routing_weight[None, :, :], axis=2)
    gate_factor = jax.nn.sigmoid(dense_gate)[:, None]
    return (routed + gate_factor * dense_out).T.astype(jnp.bfloat16)


BF = jnp.bfloat16
F32 = jnp.float32


def silu_mul(gate_act, up_act):
    return (gate_act / (1.0 + jnp.exp(-gate_act)) * up_act).astype(BF)


def dot_t(rows, weights):
    return lax.dot_general(rows, weights, (((1,), (1,)), ((), ())), preferred_element_type=F32)


SOURCES = ((3, 2, 1), (0, 3, 2), (3, 0, 1), (0, 1, 2))
TARGETS = ((3, 1, 2), (0, 3, 2), (3, 0, 1), (0, 2, 1))
SCHEDULE = (
    "N", "D", "G10", "H00", "G11", "G20", "K2", "H02", "G21", "C1", "H01", "X1", "Y1",
    "G31", "P00", "S1", "X2", "P01", "G30", "L1", "Y2", "C2", "S2", "A00", "Y3", "H11",
    "H10", "X3", "H12", "L2", "C3", "A01", "P10", "P11", "S3", "H22", "A10", "H20",
    "L3", "E0", "A11", "F0", "H21", "P20", "H32", "P21", "E1", "A20", "H30", "A21",
    "H31", "P30", "F1", "P31", "E2", "J0", "A30", "F2", "I1", "K3", "A31", "J1", "I2",
    "E3", "K1", "F3", "J2", "I3", "I0", "J3", "R1", "R2", "R3",
)


def fused_kernel(
    tok_hbm,
    gain_hbm,
    ids_hbm,
    rw_hbm,
    gw_hbm,
    uw_hbm,
    dw_hbm,
    dg_hbm,
    du_hbm,
    dd_hbm,
    dgate_hbm,
    out_ref,
    tok_ref,
    gain_ref,
    ids_ref,
    rw_ref,
    gw,
    uw,
    dw,
    dgu,
    dd,
    factor,
    normed,
    slot_row,
    slot_col,
    weight_col,
    gates,
    zsend,
    xbuf,
    hid_l,
    hid_c,
    dhid,
    part_l,
    part_c,
    r0_l,
    r0_c,
    r1a_l,
    r1b_l,
    r1a_c,
    r1b_c,
    r2a_l,
    r2b_l,
    r2a_c,
    r2b_c,
    fin,
    ret,
    chosen,
    scale_col,
    total,
    wsem,
    zsem,
    rsem,
    sems,
):
    me = lax.axis_index("ep")
    tp = lax.axis_index("tp")
    core, xx, yy = tp % 2, (tp // 2) % 2, tp // 4
    group, width = tok_ref.shape
    cols = out_ref.shape[1]
    rounds, cap = zsend.shape[:2]
    ffp = gw.shape[0]
    dsp = dd.shape[0]
    half = cap // 2
    mesh_id = pl.DeviceIdType.MESH
    to_core, to_x, to_y = 1, 2, 4

    def peer(flip):
        bits = (core + flip % 2) % 2, (xx + flip // 2 % 2) % 2, (yy + flip // 4) % 2
        return bits[2] * 4 + bits[1] * 2 + bits[0]

    place_value = (1 + 3 * (me % 2)) * (1 + 15 * (me // 2))

    def lookup(row):
        return sum(value * 4**plane for plane, value in enumerate(row)) // place_value % 4

    def source(slot):
        return lookup([row[slot - 1] for row in SOURCES])

    def slot_at(other):
        return lookup([SOURCES[q].index(p) for p, q in enumerate(other)])

    barrier = pltpu.get_barrier_semaphore()
    for flip in range(1, 8):
        pl.semaphore_signal(barrier, 1, device_id=(me, peer(flip)), device_id_type=mesh_id)
    for j in range(1, rounds + 1):
        pl.semaphore_signal(
            barrier, 1, device_id=((me + j) % 4, peer(to_core)), device_id_type=mesh_id
        )

    loads = {
        "ids": pltpu.make_async_copy(ids_hbm, ids_ref, wsem.at[6]),
        "tok": pltpu.make_async_copy(tok_hbm, tok_ref, wsem.at[7]),
        "gain": pltpu.make_async_copy(gain_hbm, gain_ref, wsem.at[8]),
        "rw": pltpu.make_async_copy(rw_hbm, rw_ref, wsem.at[9]),
        "dgate": pltpu.make_async_copy(dgate_hbm, gates.at[tp], wsem.at[10]),
        "g": pltpu.make_async_copy(gw_hbm.at[0], gw, wsem.at[0]),
        "u": pltpu.make_async_copy(uw_hbm.at[0], uw, wsem.at[1]),
        "dg": pltpu.make_async_copy(dg_hbm, dgu.at[:, pl.ds(0, dsp)], wsem.at[2]),
        "du": pltpu.make_async_copy(du_hbm, dgu.at[:, pl.ds(dsp, dsp)], wsem.at[3]),
        "d": pltpu.make_async_copy(dw_hbm.at[0], dw, wsem.at[4]),
        "dd": pltpu.make_async_copy(dd_hbm, dd, wsem.at[5]),
    }
    for load in loads.values():
        load.start()

    def need(*names):
        for name in names:
            if name in loads:
                loads.pop(name).wait()

    started, expected = [], {}

    def transfer(src, dst, send_sem, recv_sem, target):
        return pltpu.make_async_remote_copy(
            src_ref=src,
            dst_ref=dst,
            send_sem=send_sem,
            recv_sem=recv_sem,
            device_id=target,
            device_id_type=mesh_id,
        )

    def send(name, src, dst, target):
        n = len(started)
        copy = transfer(src, dst, sems.at[0, n], sems.at[1, n], target)
        copy.start()
        started.append(copy)
        expected[name] = copy

    def got(*names):
        for name in names:
            if expected[name] is not None:
                expected[name].wait_recv()
                expected[name] = None

    def hop(sem, src, dst, number, landing, h, plane):
        rows = tops[h]
        copy = transfer(
            src.at[number, rows],
            dst(landing, rows, tp),
            sem.at[0, number, h],
            sem.at[1, landing, h],
            (plane, peer(to_core)),
        )
        copy.start()
        started.append(copy)

    def z_place(slot, rows, part):
        return xbuf.at[slot, rows, span(part)]

    def r_place(slot, rows, part):
        return ret.at[slot, rows]

    def at_tp(flip):
        return (me, peer(flip))

    tops = {0: pl.ds(0, half), 1: pl.ds(half, half)}

    def span(slice_no):
        return pl.ds(pl.multiple_of(slice_no * cols, cols), cols)

    need("ids")
    id0, id1 = ids_ref[0:1, :], ids_ref[1:2, :]
    number = lax.broadcasted_iota(jnp.int32, (128, group), 0)
    named = (id0 == number) | (id1 == number)
    earlier = jnp.where(
        lax.broadcasted_iota(jnp.int32, (group, group), 0)
        < lax.broadcasted_iota(jnp.int32, (group, group), 1),
        1.0,
        0.0,
    ).astype(BF)
    marks = jnp.where(named, 1.0, 0.0).astype(BF)
    count = jnp.dot(marks, earlier, preferred_element_type=F32)
    slots = jnp.where(named, count, -1.0)
    slot_row[...] = slots

    need("tok")
    step = 64
    for i in range(0, group, step):
        values = tok_ref[i : i + step, :].astype(F32)
        mean = jnp.sum(values * values, axis=1, keepdims=True) * (1.0 / width)
        factor[i : i + step, :] = jnp.broadcast_to(lax.rsqrt(mean + EPSILON), (step, 128))

    def pick(e):
        row = slot_row[pl.ds(e, 1), :].astype(jnp.int32)
        where = lax.broadcasted_iota(jnp.int32, (cap, group), 0)
        return jnp.where(row == where, 1.0, 0.0).astype(BF)

    need("gain")
    own = (tok_ref[:, span(tp)].astype(F32) * factor[:, 0:1] * gain_ref[:, span(tp)]).astype(BF)
    for n in range(rounds):
        targets = [row[n] for row in TARGETS]
        plane = lookup(targets)
        zsend[n] = jnp.dot(pick(plane), own, preferred_element_type=F32).astype(BF)
        if n == 0:
            pl.semaphore_wait(barrier, 7 + rounds)
        for h in tops:
            hop(zsem, zsend, z_place, n, slot_at(targets), h, plane)
    for n in range(rounds):
        for h, rows in tops.items():
            for kind, sem, src, place in (("z", zsem, zsend, z_place), ("r", rsem, fin, r_place)):
                landed = place(n, rows, peer(to_core))
                expected[kind, n + 1, h] = transfer(
                    src.at[n, rows], landed, sem.at[0, n, h], sem.at[1, n, h], at_tp(to_core)
                )
    need("dgate", "rw")
    for flip in range(1, 8):
        send(("gate", flip), gates.at[tp], gates.at[tp], at_tp(flip))

    weights = jnp.where(id0 == number, rw_ref[0:1, :], 0.0) + jnp.where(id1 == number, rw_ref[1:2, :], 0.0)
    slot_col[...] = slots.T
    weight_col[...] = weights.T
    lane = lax.broadcasted_iota(jnp.int32, (group, 128), 1)

    def weight_of(e):
        return jnp.sum(jnp.where(lane == e, weight_col[...], 0.0), axis=1, keepdims=True)

    def norm_all():
        gain = gain_ref[...]

        def body(i, carry):
            rows = pl.ds(pl.multiple_of(i * 32, 32), 32)
            values = tok_ref[rows, :].astype(F32)
            normed[rows, :] = (values * factor[rows, 0:1] * gain).astype(BF)
            return carry

        lax.fori_loop(0, group // 32, body, 0)

    def forward(name, j, rows, slice_flip, flip):
        ref = xbuf.at[j - 1, rows, span(peer(slice_flip))]
        send((name, j), ref, ref, at_tp(flip))

    everything = pl.ds(0, cap)

    def gather_start(j, h):
        got(("z", j, h))
        forward("x%d" % h, j, tops[h], to_core, to_x + to_core)
        forward("y%d" % h, j, tops[h], to_core, to_y + to_core)

    def gather_core(j):
        forward("c", j, everything, to_core, to_core)

    def gather_relay_x(j):
        got(("x0", j))
        forward("xy", j, tops[0], to_x, to_y + to_core)

    def gather_relay_y(j):
        got(("y1", j))
        forward("yx", j, tops[1], to_y, to_x + to_core)

    def gather_share(j):
        got(("x0", j), ("x1", j))
        forward("xc", j, everything, to_x, to_core)
        got(("y0", j), ("y1", j))
        forward("yc", j, everything, to_y, to_core)

    def gather_last(j):
        got(("xy", j))
        forward("xyc", j, tops[0], 7, to_core)
        got(("yx", j))
        forward("yxc", j, tops[1], 7, to_core)

    tiles = [(n, min(256, ffp - n)) for n in range(0, ffp, 256)]

    def hidden_tile(b, t):
        need("g", "u")
        if b:
            got(*[(name, b) for name in ("c", "xc", "yc", "xyc", "yxc")])
        rows = xbuf[b - 1] if b else normed[...]
        n, size = tiles[t]
        value = silu_mul(dot_t(rows, gw[n : n + size, :]), dot_t(rows, uw[n : n + size, :]))
        if b:
            hid_c[b - 1, :, n : n + size] = value
        else:
            hid_l[:, n : n + size] = value

    def dense_hidden():
        need("dg", "du")
        acts = jnp.dot(normed[...], dgu[...], preferred_element_type=F32)
        dhid[...] = silu_mul(acts[:, :dsp], acts[:, dsp:])

    def rs_refs(b):
        if b == 0:
            return part_l, r0_l, r1a_l, r1b_l, r2a_l, r2b_l
        return tuple(r.at[b - 1] for r in (part_c, r0_c, r1a_c, r1b_c, r2a_c, r2b_c))

    def halves(b):
        h = (cap if b else group) // 2
        return pl.ds(0, h), pl.ds(h, h)

    def partial(b, mine):
        need("d", "dd")
        half_no = 0 if mine else 1
        swap = half_no + (1 if b else 0)
        part, r0 = rs_refs(b)[:2]
        if b == 0:
            scale = weight_of(me)
            got(*[("gate", flip) for flip in range(1, 8)])
        corners = ((1 - yy, 1 - xx), (yy, 1 - xx), (1 - yy, xx), (yy, xx))
        for (y, x), odd in zip(corners, (0, 1, 1, 0)):
            k = 4 * y + 2 * x + (core + odd + swap) % 2
            if b:
                value = jnp.dot(hid_c[b - 1], dw[:, span(k)], preferred_element_type=F32)
            else:
                side = jnp.dot(dhid[...], dd[:, span(k)], preferred_element_type=F32)
                value = jnp.dot(hid_l[...], dw[:, span(k)], preferred_element_type=F32)
                value = scale * value + jax.nn.sigmoid(gates[k]) * side
            part[half_no, y, x] = value.astype(BF)
        if not mine:
            for q, (y, x) in enumerate(corners):
                send(("r0", q, b), part.at[half_no, y, x], r0.at[y, x], at_tp(to_core))

    def add(dst, index, other):
        dst[index] = (dst[index].astype(F32) + other.astype(F32)).astype(BF)

    def scatter_one(b, late):
        part, r0, r1a, r1b = rs_refs(b)[:4]
        top, bottom = halves(b)
        if not late:
            got(("r0", 0, b))
            add(part, (0, 1 - yy, 1 - xx), r0[1 - yy, 1 - xx])
            send(("a0", b), part.at[0, 1 - yy, 1 - xx, top], r1a.at[1 - yy], at_tp(to_x + to_core))
            send(("b0", b), part.at[0, 1 - yy, 1 - xx, bottom], r1b.at[1 - xx], at_tp(to_y + to_core))
        else:
            got(("r0", 1, b))
            add(part, (0, yy, 1 - xx), r0[yy, 1 - xx])
            send(("a1", b), part.at[0, yy, 1 - xx, top], r1a.at[yy], at_tp(to_x + to_core))
            got(("r0", 2, b))
            add(part, (0, 1 - yy, xx), r0[1 - yy, xx])
            send(("b1", b), part.at[0, 1 - yy, xx, bottom], r1b.at[xx], at_tp(to_y + to_core))

    def scatter_two_a(b):
        part, r0, r1a, r1b, r2a, r2b = rs_refs(b)
        top, bottom = halves(b)
        got(("a0", b))
        add(part, (0, 1 - yy, xx, top), r1a[1 - yy])
        send(("a2", b), part.at[0, 1 - yy, xx, top], r2a, at_tp(to_y + to_core))

    def scatter_two_b(b):
        part, r0, r1a, r1b, r2a, r2b = rs_refs(b)
        top, bottom = halves(b)
        got(("b0", b))
        add(part, (0, yy, 1 - xx, bottom), r1b[1 - xx])
        send(("b2", b), part.at[0, yy, 1 - xx, bottom], r2b, at_tp(to_x + to_core))

    def finish(b, h, value):
        rows = halves(b)[h]
        if b == 0:
            total[rows, :] = value
        else:
            fin[b - 1, rows, :] = value.astype(BF)
            sources = [row[b - 1] for row in SOURCES]
            hop(rsem, fin, r_place, b - 1, slot_at(sources), h, source(b))

    def scatter_three_a(b):
        part, r0, r1a, r1b, r2a, r2b = rs_refs(b)
        rows = halves(b)[0]
        got(("r0", 3, b), ("a1", b), ("a2", b))
        mine = part[0, yy, xx, rows].astype(F32) + r0[yy, xx, rows].astype(F32)
        finish(b, 0, mine + r1a[yy].astype(F32) + r2a[...].astype(F32))

    def scatter_three_b(b):
        part, r0, r1a, r1b, r2a, r2b = rs_refs(b)
        rows = halves(b)[1]
        got(("r0", 3, b), ("b1", b), ("b2", b))
        mine = part[0, yy, xx, rows].astype(F32) + r0[yy, xx, rows].astype(F32)
        finish(b, 1, mine + r1b[xx].astype(F32) + r2b[...].astype(F32))

    def prepare(j):
        e = source(j)
        slot = jnp.sum(jnp.where(lane == e, slot_col[...], 0.0), axis=1, keepdims=True).astype(jnp.int32)
        where = lax.broadcasted_iota(jnp.int32, (group, cap), 1)
        chosen[j - 1] = jnp.where(slot == where, 1.0, 0.0).astype(BF)
        scale_col[j - 1] = jnp.broadcast_to(weight_of(e), (group, 128))

    def returned(j):
        got(("r", j, 0), ("r", j, 1))
        rows = jnp.dot(chosen[j - 1], ret[j - 1], preferred_element_type=F32)
        value = total[...] + scale_col[j - 1][:, 0:1] * rows
        if ("R%d" % j) == SCHEDULE[-1]:
            out_ref[...] = value.astype(BF)
        else:
            total[...] = value

    steps = {
        "N": norm_all,
        "G": gather_start,
        "C": gather_core,
        "X": gather_relay_x,
        "Y": gather_relay_y,
        "S": gather_share,
        "L": gather_last,
        "H": hidden_tile,
        "D": dense_hidden,
        "P": partial,
        "A": scatter_one,
        "E": scatter_two_a,
        "F": scatter_two_b,
        "I": scatter_three_a,
        "J": scatter_three_b,
        "K": prepare,
        "R": returned,
    }
    for word in SCHEDULE:
        steps[word[0]](*[int(digit) for digit in word[1:]])
    for copy in started:
        copy.wait_send()


def fused_local(
    tokens,
    norm_gain,
    expert_ids,
    routing_weight,
    expert_gate,
    expert_up,
    expert_down,
    dense_gate_w,
    dense_up_w,
    dense_down_w,
    dense_gate,
):
    experts = lax.axis_size("ep")
    parts = lax.axis_size("tp")
    group, width = tokens.shape
    cap = 3 * group // experts
    cols = width // parts
    ffp = expert_gate.shape[2]
    dsp = dense_gate_w.shape[1]
    rounds = experts - 1
    vmem, hbm = pl.BlockSpec(memory_space=pltpu.VMEM), pl.BlockSpec(memory_space=pl.ANY)
    dma = pltpu.SemaphoreType.DMA
    half, ghalf = cap // 2, group // 2
    return pl.pallas_call(
        fused_kernel,
        out_shape=pltpu.VMEM((group, cols), BF),
        in_specs=[hbm] * 11,
        out_specs=vmem,
        scratch_shapes=[
            pltpu.VMEM((group, width), BF),
            pltpu.VMEM((1, width), F32),
            pltpu.VMEM((2, group), jnp.int32),
            pltpu.VMEM((2, group), F32),
            pltpu.VMEM((ffp, width), BF),
            pltpu.VMEM((ffp, width), BF),
            pltpu.VMEM((ffp, width), BF),
            pltpu.VMEM((width, 2 * dsp), BF),
            pltpu.VMEM((dsp, width), BF),
            pltpu.VMEM((group, 128), F32),
            pltpu.VMEM((group, width), BF),
            pltpu.VMEM((128, group), F32),
            pltpu.VMEM((group, 128), F32),
            pltpu.VMEM((group, 128), F32),
            pltpu.VMEM((parts, 1, cols), F32),
            pltpu.VMEM((rounds, cap, cols), BF),
            pltpu.VMEM((rounds, cap, width), BF),
            pltpu.VMEM((group, ffp), BF),
            pltpu.VMEM((rounds, cap, ffp), BF),
            pltpu.VMEM((group, dsp), BF),
            pltpu.VMEM((2, 2, 2, group, cols), BF),
            pltpu.VMEM((rounds, 2, 2, 2, cap, cols), BF),
            pltpu.VMEM((2, 2, group, cols), BF),
            pltpu.VMEM((rounds, 2, 2, cap, cols), BF),
            pltpu.VMEM((2, ghalf, cols), BF),
            pltpu.VMEM((2, ghalf, cols), BF),
            pltpu.VMEM((rounds, 2, half, cols), BF),
            pltpu.VMEM((rounds, 2, half, cols), BF),
            pltpu.VMEM((ghalf, cols), BF),
            pltpu.VMEM((ghalf, cols), BF),
            pltpu.VMEM((rounds, half, cols), BF),
            pltpu.VMEM((rounds, half, cols), BF),
            pltpu.VMEM((rounds, cap, cols), BF),
            pltpu.VMEM((rounds, cap, cols), BF),
            pltpu.VMEM((rounds, group, cap), BF),
            pltpu.VMEM((rounds, group, 128), F32),
            pltpu.VMEM((group, cols), F32),
            dma((11,)),
            dma((2, rounds, 2)),
            dma((2, rounds, 2)),
            dma((2, 92)),
        ],
        compiler_params=pltpu.CompilerParams(
            collective_id=0, has_side_effects=True, vmem_limit_bytes=56 * 1024 * 1024
        ),
        name="routed_layer",
    )(
        tokens,
        norm_gain[None, :],
        expert_ids.T,
        routing_weight.T,
        jnp.swapaxes(expert_gate, 1, 2),
        jnp.swapaxes(expert_up, 1, 2),
        expert_down,
        dense_gate_w,
        dense_up_w,
        dense_down_w,
        dense_gate[None, :],
    )


def local(*args):
    experts, parts = lax.axis_size("ep"), lax.axis_size("tp")
    group, width = args[0].shape
    fits = (
        experts == 4
        and parts == 8
        and width % (128 * parts) == 0
        and group % 128 == 0
        and (3 * group // experts) % 32 == 0
        and args[7].shape[1] % 128 == 0
        and args[4].shape[2] % 16 == 0
    )
    return (fused_local if fits else plain_local)(*args)


def solution(mesh):
    return jax.shard_map(
        local,
        mesh=mesh,
        in_specs=(
            P("ep", None),
            P(),
            P("ep", None),
            P("ep", None),
            P("ep", None, "tp"),
            P("ep", None, "tp"),
            P("ep", "tp", None),
            P(None, "tp"),
            P(None, "tp"),
            P("tp", None),
            P("tp"),
        ),
        out_specs=P("ep", "tp"),
        check_vma=False,
    )
```

```python
import jax
import jax.numpy as jnp
from jax import lax
from jax.experimental import pallas as pl
from jax.experimental.pallas import tpu as pltpu
from jax.sharding import PartitionSpec as P

EPSILON = 1e-06


def positions(block_ids, experts, capacity):
    flat_ids = block_ids.reshape(-1)
    one_hot = (flat_ids[:, None] == jnp.arange(experts, dtype=jnp.int32)[None, :]).astype(jnp.int32)
    earlier = jnp.cumsum(one_hot, axis=0) - one_hot
    return flat_ids * capacity + jnp.sum(earlier * one_hot, axis=1)


def transposed_term(hidden, down_w):
    return lax.dot_general(
        down_w, hidden, (((0,), (1,)), ((), ())), preferred_element_type=jnp.float32
    )


def plain_local(
    tokens,
    norm_gain,
    expert_ids,
    routing_weight,
    expert_gate,
    expert_up,
    expert_down,
    dense_gate_w,
    dense_up_w,
    dense_down_w,
    dense_gate,
):
    experts = lax.axis_size("ep")
    group_tokens, model_width = tokens.shape
    capacity = 3 * group_tokens // experts
    slots_all = experts * capacity
    part_rows = model_width // lax.axis_size("tp")
    values = tokens.astype(jnp.float32)
    factor = lax.rsqrt(jnp.mean(values * values, axis=-1, keepdims=True) + EPSILON)
    normed = (values * factor * norm_gain[None, :]).astype(jnp.bfloat16)
    places = positions(expert_ids, experts, capacity)
    token_no = jnp.arange(2 * group_tokens, dtype=jnp.int32) // 2 + 1
    sources = jnp.zeros((slots_all,), jnp.int32).at[places].set(token_no)
    padded = jnp.concatenate([jnp.zeros((1, model_width), jnp.bfloat16), normed], axis=0)
    gate_w = expert_gate[0]
    up_w = expert_up[0]
    down_w = expert_down[0]
    first_col = lax.axis_index("tp") * part_rows
    column_part = lax.dynamic_slice_in_dim(padded, first_col, part_rows, 1)
    outgoing = column_part[sources].reshape(experts, capacity, part_rows)
    landed = lax.all_to_all(outgoing, "ep", split_axis=0, concat_axis=0, tiled=True)
    portion = lax.all_gather(landed, "tp", axis=2, tiled=True)
    columns = portion.reshape(slots_all, portion.shape[2])
    gate_act = jnp.dot(columns, gate_w, preferred_element_type=jnp.float32)
    up_act = jnp.dot(columns, up_w, preferred_element_type=jnp.float32)
    hidden = (jax.nn.silu(gate_act) * up_act).astype(jnp.bfloat16)
    dense_gate_act = jnp.dot(normed, dense_gate_w, preferred_element_type=jnp.float32)
    dense_up_act = jnp.dot(normed, dense_up_w, preferred_element_type=jnp.float32)
    dense_hidden = (jax.nn.silu(dense_gate_act) * dense_up_act).astype(jnp.bfloat16)
    dense_out = lax.psum_scatter(
        transposed_term(dense_hidden, dense_down_w).astype(jnp.bfloat16),
        "tp",
        scatter_dimension=0,
        tiled=True,
    ).astype(jnp.float32)
    expert_out = lax.psum_scatter(
        transposed_term(hidden, down_w).astype(jnp.bfloat16), "tp", scatter_dimension=0, tiled=True
    )
    expert_half = expert_out.reshape(part_rows, experts, capacity)
    returned = lax.all_to_all(expert_half, "ep", split_axis=1, concat_axis=1, tiled=True).reshape(
        part_rows, slots_all
    )
    picked = (
        jnp.take(returned, places, axis=1).astype(jnp.float32).reshape(part_rows, group_tokens, 2)
    )
    routed = jnp.sum(picked * routing_weight[None, :, :], axis=2)
    gate_factor = jax.nn.sigmoid(dense_gate)[:, None]
    return (routed + gate_factor * dense_out).T.astype(jnp.bfloat16)


BF = jnp.bfloat16
F32 = jnp.float32


def silu_mul(gate_act, up_act):
    return (gate_act / (1.0 + jnp.exp(-gate_act)) * up_act).astype(BF)


def dot_t(rows, weights):
    return lax.dot_general(rows, weights, (((1,), (1,)), ((), ())), preferred_element_type=F32)


SOURCES = ((3, 2, 1), (0, 3, 2), (3, 0, 1), (0, 1, 2))
TARGETS = ((3, 1, 2), (0, 3, 2), (3, 0, 1), (0, 2, 1))
SCHEDULE = (
    "N", "H0", "G10", "D", "G11", "G20", "G21", "X1", "W", "P00", "Y1", "C1", "P01",
    "G31", "X2", "G30", "Y2", "S1", "C3", "L1", "A00", "S2", "H1", "C2", "Y3", "X3",
    "L2", "P10", "K2", "S3", "K1", "P11", "A10", "A01", "H2", "L3", "P20", "A11", "P21",
    "K3", "F1", "A20", "E1", "H3", "A21", "P30", "P31", "F2", "A30", "J1", "E2", "A31",
    "I1", "J2", "F3", "E3", "E0", "F0", "I2", "J3", "I3", "J0", "I0", "R1", "R3", "R2",
)


def fused_kernel(
    tok_hbm,
    gain_hbm,
    ids_hbm,
    rw_hbm,
    gw_hbm,
    uw_hbm,
    dw_hbm,
    dg_hbm,
    du_hbm,
    dd_hbm,
    dgate_hbm,
    out_ref,
    tok_ref,
    gain_ref,
    ids_ref,
    rw_ref,
    gw,
    uw,
    dw,
    dgu,
    dd,
    factor,
    normed,
    slot_row,
    slot_col,
    weight_col,
    gates,
    zsend,
    xbuf,
    hid_l,
    hid_c,
    dhid,
    part_l,
    part_c,
    r0_l,
    r0_c,
    r1a_l,
    r1b_l,
    r1a_c,
    r1b_c,
    r2a_l,
    r2b_l,
    r2a_c,
    r2b_c,
    fin,
    ret,
    chosen,
    scale_col,
    total,
    wsem,
    zsem,
    rsem,
    sems,
):
    me = lax.axis_index("ep")
    tp = lax.axis_index("tp")
    core, xx, yy = tp % 2, (tp // 2) % 2, tp // 4
    group, width = tok_ref.shape
    cols = out_ref.shape[1]
    rounds, cap = zsend.shape[:2]
    ffp = gw.shape[0]
    dsp = dd.shape[0]
    half = cap // 2
    mesh_id = pl.DeviceIdType.MESH
    to_core, to_x, to_y = 1, 2, 4

    def peer(flip):
        bits = (core + flip % 2) % 2, (xx + flip // 2 % 2) % 2, (yy + flip // 4) % 2
        return bits[2] * 4 + bits[1] * 2 + bits[0]

    place_value = (1 + 3 * (me % 2)) * (1 + 15 * (me // 2))

    def lookup(row):
        return sum(value * 4**plane for plane, value in enumerate(row)) // place_value % 4

    def source(slot):
        return lookup([row[slot - 1] for row in SOURCES])

    def slot_at(other):
        return lookup([SOURCES[q].index(p) for p, q in enumerate(other)])

    barrier = pltpu.get_barrier_semaphore()
    for flip in range(1, 8):
        pl.semaphore_signal(barrier, 1, device_id=(me, peer(flip)), device_id_type=mesh_id)
    for j in range(1, rounds + 1):
        pl.semaphore_signal(
            barrier, 1, device_id=((me + j) % 4, peer(to_core)), device_id_type=mesh_id
        )

    loads = {
        "ids": pltpu.make_async_copy(ids_hbm, ids_ref, wsem.at[6]),
        "gain": pltpu.make_async_copy(gain_hbm, gain_ref, wsem.at[8]),
        "rw": pltpu.make_async_copy(rw_hbm, rw_ref, wsem.at[9]),
        "dgate": pltpu.make_async_copy(dgate_hbm, gates.at[tp], wsem.at[10]),
        "g": pltpu.make_async_copy(gw_hbm.at[0], gw, wsem.at[0]),
        "u": pltpu.make_async_copy(uw_hbm.at[0], uw, wsem.at[1]),
        "dg": pltpu.make_async_copy(dg_hbm, dgu.at[:, pl.ds(0, dsp)], wsem.at[2]),
        "du": pltpu.make_async_copy(du_hbm, dgu.at[:, pl.ds(dsp, dsp)], wsem.at[3]),
        "d": pltpu.make_async_copy(dw_hbm.at[0], dw, wsem.at[4]),
        "dd": pltpu.make_async_copy(dd_hbm, dd, wsem.at[5]),
    }
    step = group // 4
    for i in range(4):
        rows = pl.ds(i * step, step)
        copy = pltpu.make_async_copy(tok_hbm.at[rows], tok_ref.at[rows], wsem.at[11 + i])
        loads = {"tok%d" % i: copy, **loads}
    loads = {"ids": loads.pop("ids"), **{"tok%d" % i: loads["tok%d" % i] for i in range(4)}, **loads}
    for load in loads.values():
        load.start()

    def need(*names):
        for name in names:
            if name in loads:
                loads.pop(name).wait()

    started, expected = [], {}

    def transfer(src, dst, send_sem, recv_sem, target):
        return pltpu.make_async_remote_copy(
            src_ref=src,
            dst_ref=dst,
            send_sem=send_sem,
            recv_sem=recv_sem,
            device_id=target,
            device_id_type=mesh_id,
        )

    def send(name, src, dst, target):
        n = len(started)
        copy = transfer(src, dst, sems.at[0, n], sems.at[1, n], target)
        copy.start()
        started.append(copy)
        expected[name] = copy

    def got(*names):
        for name in names:
            if expected[name] is not None:
                expected[name].wait_recv()
                expected[name] = None

    def hop(sem, src, dst, number, landing, h, plane):
        rows = tops[h]
        copy = transfer(
            src.at[number, rows],
            dst(landing, rows, tp),
            sem.at[0, number, h],
            sem.at[1, landing, h],
            (plane, peer(to_core)),
        )
        copy.start()
        started.append(copy)

    def z_place(slot, rows, part):
        return xbuf.at[slot, rows, span(part)]

    def r_place(slot, rows, part):
        return ret.at[slot, rows]

    def at_tp(flip):
        return (me, peer(flip))

    tops = {0: pl.ds(0, half), 1: pl.ds(half, half)}

    def span(slice_no):
        return pl.ds(pl.multiple_of(slice_no * cols, cols), cols)

    number = lax.broadcasted_iota(jnp.int32, (128, group), 0)
    earlier = jnp.where(
        lax.broadcasted_iota(jnp.int32, (group, group), 0)
        < lax.broadcasted_iota(jnp.int32, (group, group), 1),
        1.0,
        0.0,
    ).astype(BF)
    need("ids")
    id0, id1 = ids_ref[0:1, :], ids_ref[1:2, :]
    named = (id0 == number) | (id1 == number)
    marks = jnp.where(named, 1.0, 0.0).astype(BF)
    count = jnp.dot(marks, earlier, preferred_element_type=F32)
    slots = jnp.where(named, count, -1.0)
    slot_row[...] = slots

    for i in range(4):
        need("tok%d" % i)
        rows = pl.ds(i * step, step)
        values = tok_ref[rows, :].astype(F32)
        mean = jnp.sum(values * values, axis=1, keepdims=True) * (1.0 / width)
        factor[rows, :] = jnp.broadcast_to(lax.rsqrt(mean + EPSILON), (step, 128))

    def pick(e):
        row = slot_row[pl.ds(e, 1), :].astype(jnp.int32)
        where = lax.broadcasted_iota(jnp.int32, (cap, group), 0)
        return jnp.where(row == where, 1.0, 0.0).astype(BF)

    need("gain")
    own = (tok_ref[:, span(tp)].astype(F32) * factor[:, 0:1] * gain_ref[:, span(tp)]).astype(BF)
    for n in range(rounds):
        targets = [row[n] for row in TARGETS]
        plane = lookup(targets)
        zsend[n] = jnp.dot(pick(plane), own, preferred_element_type=F32).astype(BF)
        if n == 0:
            pl.semaphore_wait(barrier, 7 + rounds)
        for h in tops:
            hop(zsem, zsend, z_place, n, slot_at(targets), h, plane)
    for n in range(rounds):
        for h, rows in tops.items():
            for kind, sem, src, place in (("z", zsem, zsend, z_place), ("r", rsem, fin, r_place)):
                landed = place(n, rows, peer(to_core))
                expected[kind, n + 1, h] = transfer(
                    src.at[n, rows], landed, sem.at[0, n, h], sem.at[1, n, h], at_tp(to_core)
                )
    need("dgate", "rw")
    for flip in range(1, 8):
        send(("gate", flip), gates.at[tp], gates.at[tp], at_tp(flip))

    weights = jnp.where(id0 == number, rw_ref[0:1, :], 0.0) + jnp.where(id1 == number, rw_ref[1:2, :], 0.0)
    slot_col[...] = slots.T
    weight_col[...] = weights.T
    lane = lax.broadcasted_iota(jnp.int32, (group, 128), 1)

    def weight_of(e):
        return jnp.sum(jnp.where(lane == e, weight_col[...], 0.0), axis=1, keepdims=True)

    def norm_all():
        gain = gain_ref[...]

        def body(i, carry):
            rows = pl.ds(pl.multiple_of(i * 32, 32), 32)
            values = tok_ref[rows, :].astype(F32)
            normed[rows, :] = (values * factor[rows, 0:1] * gain).astype(BF)
            return carry

        lax.fori_loop(0, group // 32, body, 0)

    def forward(name, j, rows, slice_flip, flip):
        ref = xbuf.at[j - 1, rows, span(peer(slice_flip))]
        send((name, j), ref, ref, at_tp(flip))

    everything = pl.ds(0, cap)

    def gather_start(j, h):
        got(("z", j, h))
        forward("x%d" % h, j, tops[h], to_core, to_x + to_core)
        forward("y%d" % h, j, tops[h], to_core, to_y + to_core)

    def gather_core(j):
        forward("c", j, everything, to_core, to_core)

    def gather_relay_x(j):
        got(("x0", j))
        forward("xy", j, tops[0], to_x, to_y + to_core)

    def gather_relay_y(j):
        got(("y1", j))
        forward("yx", j, tops[1], to_y, to_x + to_core)

    def gather_share(j):
        got(("x0", j), ("x1", j))
        forward("xc", j, everything, to_x, to_core)
        got(("y0", j), ("y1", j))
        forward("yc", j, everything, to_y, to_core)

    def gather_last(j):
        got(("xy", j))
        forward("xyc", j, tops[0], 7, to_core)
        got(("yx", j))
        forward("yxc", j, tops[1], 7, to_core)

    def hidden(b):
        need("g", "u")
        if b:
            got(*[(name, b) for name in ("c", "xc", "yc", "xyc", "yxc")])
        rows = xbuf[b - 1] if b else normed[...]
        value = silu_mul(dot_t(rows, gw[...]), dot_t(rows, uw[...]))
        if b:
            hid_c[b - 1] = value
        else:
            hid_l[...] = value

    def local_scale():
        scale_col[rounds] = jnp.broadcast_to(weight_of(me), (group, 128))

    def dense_hidden():
        need("dg", "du")
        both = jnp.dot(normed[...], dgu[...], preferred_element_type=F32)
        dhid[...] = silu_mul(both[:, :dsp], both[:, dsp:])

    def rs_refs(b):
        if b == 0:
            return part_l, r0_l, r1a_l, r1b_l, r2a_l, r2b_l
        return tuple(r.at[b - 1] for r in (part_c, r0_c, r1a_c, r1b_c, r2a_c, r2b_c))

    def halves(b):
        h = (cap if b else group) // 2
        return pl.ds(0, h), pl.ds(h, h)

    def partial(b, mine):
        need("d", "dd")
        half_no = 0 if mine else 1
        swap = half_no + (1 if b else 0)
        part, r0 = rs_refs(b)[:2]
        if b == 0:
            scale = scale_col[rounds][:, 0:1]
            got(*[("gate", flip) for flip in range(1, 8)])
        corners = ((1 - yy, 1 - xx), (yy, 1 - xx), (1 - yy, xx), (yy, xx))
        for (y, x), odd in zip(corners, (0, 1, 1, 0)):
            k = 4 * y + 2 * x + (core + odd + swap) % 2
            if b:
                value = jnp.dot(hid_c[b - 1], dw[:, span(k)], preferred_element_type=F32)
            else:
                side = jnp.dot(dhid[...], dd[:, span(k)], preferred_element_type=F32)
                value = jnp.dot(hid_l[...], dw[:, span(k)], preferred_element_type=F32)
                value = scale * value + jax.nn.sigmoid(gates[k]) * side
            part[half_no, y, x] = value.astype(BF)
        if not mine:
            for q, (y, x) in enumerate(corners):
                send(("r0", q, b), part.at[half_no, y, x], r0.at[y, x], at_tp(to_core))

    def add(dst, index, other):
        dst[index] = (dst[index].astype(F32) + other.astype(F32)).astype(BF)

    def scatter_one(b, late):
        part, r0, r1a, r1b = rs_refs(b)[:4]
        top, bottom = halves(b)
        if not late:
            got(("r0", 0, b))
            add(part, (0, 1 - yy, 1 - xx), r0[1 - yy, 1 - xx])
            send(("a0", b), part.at[0, 1 - yy, 1 - xx, top], r1a.at[1 - yy], at_tp(to_x + to_core))
            send(("b0", b), part.at[0, 1 - yy, 1 - xx, bottom], r1b.at[1 - xx], at_tp(to_y + to_core))
        else:
            got(("r0", 1, b))
            add(part, (0, yy, 1 - xx), r0[yy, 1 - xx])
            send(("a1", b), part.at[0, yy, 1 - xx, top], r1a.at[yy], at_tp(to_x + to_core))
            got(("r0", 2, b))
            add(part, (0, 1 - yy, xx), r0[1 - yy, xx])
            send(("b1", b), part.at[0, 1 - yy, xx, bottom], r1b.at[xx], at_tp(to_y + to_core))

    def scatter_two_a(b):
        part, r0, r1a, r1b, r2a, r2b = rs_refs(b)
        top, bottom = halves(b)
        got(("a0", b))
        add(part, (0, 1 - yy, xx, top), r1a[1 - yy])
        send(("a2", b), part.at[0, 1 - yy, xx, top], r2a, at_tp(to_y + to_core))

    def scatter_two_b(b):
        part, r0, r1a, r1b, r2a, r2b = rs_refs(b)
        top, bottom = halves(b)
        got(("b0", b))
        add(part, (0, yy, 1 - xx, bottom), r1b[1 - xx])
        send(("b2", b), part.at[0, yy, 1 - xx, bottom], r2b, at_tp(to_x + to_core))

    def finish(b, h, value):
        rows = halves(b)[h]
        if b == 0:
            total[rows, :] = value
        else:
            fin[b - 1, rows, :] = value.astype(BF)
            sources = [row[b - 1] for row in SOURCES]
            hop(rsem, fin, r_place, b - 1, slot_at(sources), h, source(b))

    def scatter_three_a(b):
        part, r0, r1a, r1b, r2a, r2b = rs_refs(b)
        rows = halves(b)[0]
        got(("r0", 3, b), ("a1", b), ("a2", b))
        mine = part[0, yy, xx, rows].astype(F32) + r0[yy, xx, rows].astype(F32)
        finish(b, 0, mine + r1a[yy].astype(F32) + r2a[...].astype(F32))

    def scatter_three_b(b):
        part, r0, r1a, r1b, r2a, r2b = rs_refs(b)
        rows = halves(b)[1]
        got(("r0", 3, b), ("b1", b), ("b2", b))
        mine = part[0, yy, xx, rows].astype(F32) + r0[yy, xx, rows].astype(F32)
        finish(b, 1, mine + r1b[xx].astype(F32) + r2b[...].astype(F32))

    def prepare(j):
        e = source(j)
        slot = jnp.sum(jnp.where(lane == e, slot_col[...], 0.0), axis=1, keepdims=True).astype(jnp.int32)
        where = lax.broadcasted_iota(jnp.int32, (group, cap), 1)
        chosen[j - 1] = jnp.where(slot == where, 1.0, 0.0).astype(BF)
        scale_col[j - 1] = jnp.broadcast_to(weight_of(e), (group, 128))

    def returned(j):
        got(("r", j, 0), ("r", j, 1))
        rows = jnp.dot(chosen[j - 1], ret[j - 1], preferred_element_type=F32)
        value = total[...] + scale_col[j - 1][:, 0:1] * rows
        if ("R%d" % j) == SCHEDULE[-1]:
            out_ref[...] = value.astype(BF)
        else:
            total[...] = value

    steps = {
        "N": norm_all,
        "G": gather_start,
        "C": gather_core,
        "X": gather_relay_x,
        "Y": gather_relay_y,
        "S": gather_share,
        "L": gather_last,
        "H": hidden,
        "W": local_scale,
        "D": dense_hidden,
        "P": partial,
        "A": scatter_one,
        "E": scatter_two_a,
        "F": scatter_two_b,
        "I": scatter_three_a,
        "J": scatter_three_b,
        "K": prepare,
        "R": returned,
    }
    for word in SCHEDULE:
        steps[word[0]](*[int(digit) for digit in word[1:]])
    for copy in started:
        copy.wait_send()


def fused_local(
    tokens,
    norm_gain,
    expert_ids,
    routing_weight,
    expert_gate,
    expert_up,
    expert_down,
    dense_gate_w,
    dense_up_w,
    dense_down_w,
    dense_gate,
):
    experts = lax.axis_size("ep")
    parts = lax.axis_size("tp")
    group, width = tokens.shape
    cap = 3 * group // experts
    cols = width // parts
    ffp = expert_gate.shape[2]
    dsp = dense_gate_w.shape[1]
    rounds = experts - 1
    vmem, hbm = pl.BlockSpec(memory_space=pltpu.VMEM), pl.BlockSpec(memory_space=pl.ANY)
    dma = pltpu.SemaphoreType.DMA
    half, ghalf = cap // 2, group // 2
    return pl.pallas_call(
        fused_kernel,
        out_shape=pltpu.VMEM((group, cols), BF),
        in_specs=[hbm] * 11,
        out_specs=vmem,
        scratch_shapes=[
            pltpu.VMEM((group, width), BF),
            pltpu.VMEM((1, width), F32),
            pltpu.VMEM((2, group), jnp.int32),
            pltpu.VMEM((2, group), F32),
            pltpu.VMEM((ffp, width), BF),
            pltpu.VMEM((ffp, width), BF),
            pltpu.VMEM((ffp, width), BF),
            pltpu.VMEM((width, 2 * dsp), BF),
            pltpu.VMEM((dsp, width), BF),
            pltpu.VMEM((group, 128), F32),
            pltpu.VMEM((group, width), BF),
            pltpu.VMEM((128, group), F32),
            pltpu.VMEM((group, 128), F32),
            pltpu.VMEM((group, 128), F32),
            pltpu.VMEM((parts, 1, cols), F32),
            pltpu.VMEM((rounds, cap, cols), BF),
            pltpu.VMEM((rounds, cap, width), BF),
            pltpu.VMEM((group, ffp), BF),
            pltpu.VMEM((rounds, cap, ffp), BF),
            pltpu.VMEM((group, dsp), BF),
            pltpu.VMEM((2, 2, 2, group, cols), BF),
            pltpu.VMEM((rounds, 2, 2, 2, cap, cols), BF),
            pltpu.VMEM((2, 2, group, cols), BF),
            pltpu.VMEM((rounds, 2, 2, cap, cols), BF),
            pltpu.VMEM((2, ghalf, cols), BF),
            pltpu.VMEM((2, ghalf, cols), BF),
            pltpu.VMEM((rounds, 2, half, cols), BF),
            pltpu.VMEM((rounds, 2, half, cols), BF),
            pltpu.VMEM((ghalf, cols), BF),
            pltpu.VMEM((ghalf, cols), BF),
            pltpu.VMEM((rounds, half, cols), BF),
            pltpu.VMEM((rounds, half, cols), BF),
            pltpu.VMEM((rounds, cap, cols), BF),
            pltpu.VMEM((rounds, cap, cols), BF),
            pltpu.VMEM((rounds, group, cap), BF),
            pltpu.VMEM((rounds + 1, group, 128), F32),
            pltpu.VMEM((group, cols), F32),
            dma((15,)),
            dma((2, rounds, 2)),
            dma((2, rounds, 2)),
            dma((2, 92)),
        ],
        compiler_params=pltpu.CompilerParams(
            collective_id=0, has_side_effects=True, vmem_limit_bytes=56 * 1024 * 1024
        ),
        name="routed_layer",
    )(
        tokens,
        norm_gain[None, :],
        expert_ids.T,
        routing_weight.T,
        jnp.swapaxes(expert_gate, 1, 2),
        jnp.swapaxes(expert_up, 1, 2),
        expert_down,
        dense_gate_w,
        dense_up_w,
        dense_down_w,
        dense_gate[None, :],
    )


def local(*args):
    experts, parts = lax.axis_size("ep"), lax.axis_size("tp")
    group, width = args[0].shape
    fits = (
        experts == 4
        and parts == 8
        and width % (128 * parts) == 0
        and group % 128 == 0
        and (3 * group // experts) % 32 == 0
        and args[7].shape[1] % 128 == 0
        and args[4].shape[2] % 16 == 0
    )
    return (fused_local if fits else plain_local)(*args)


def solution(mesh):
    return jax.shard_map(
        local,
        mesh=mesh,
        in_specs=(
            P("ep", None),
            P(),
            P("ep", None),
            P("ep", None),
            P("ep", None, "tp"),
            P("ep", None, "tp"),
            P("ep", "tp", None),
            P(None, "tp"),
            P(None, "tp"),
            P("tp", None),
            P("tp"),
        ),
        out_specs=P("ep", "tp"),
        check_vma=False,
    )
```

```python
import jax
import jax.numpy as jnp
from jax import lax
from jax.experimental import pallas as pl
from jax.experimental.pallas import tpu as pltpu
from jax.sharding import PartitionSpec as P

EPSILON = 1e-06


def positions(block_ids, experts, capacity):
    flat_ids = block_ids.reshape(-1)
    one_hot = (flat_ids[:, None] == jnp.arange(experts, dtype=jnp.int32)[None, :]).astype(jnp.int32)
    earlier = jnp.cumsum(one_hot, axis=0) - one_hot
    return flat_ids * capacity + jnp.sum(earlier * one_hot, axis=1)


def transposed_term(hidden, down_w):
    return lax.dot_general(
        down_w, hidden, (((0,), (1,)), ((), ())), preferred_element_type=jnp.float32
    )


def plain_local(
    tokens,
    norm_gain,
    expert_ids,
    routing_weight,
    expert_gate,
    expert_up,
    expert_down,
    dense_gate_w,
    dense_up_w,
    dense_down_w,
    dense_gate,
):
    experts = lax.axis_size("ep")
    group_tokens, model_width = tokens.shape
    capacity = 3 * group_tokens // experts
    slots_all = experts * capacity
    part_rows = model_width // lax.axis_size("tp")
    values = tokens.astype(jnp.float32)
    factor = lax.rsqrt(jnp.mean(values * values, axis=-1, keepdims=True) + EPSILON)
    normed = (values * factor * norm_gain[None, :]).astype(jnp.bfloat16)
    places = positions(expert_ids, experts, capacity)
    token_no = jnp.arange(2 * group_tokens, dtype=jnp.int32) // 2 + 1
    sources = jnp.zeros((slots_all,), jnp.int32).at[places].set(token_no)
    padded = jnp.concatenate([jnp.zeros((1, model_width), jnp.bfloat16), normed], axis=0)
    gate_w = expert_gate[0]
    up_w = expert_up[0]
    down_w = expert_down[0]
    first_col = lax.axis_index("tp") * part_rows
    column_part = lax.dynamic_slice_in_dim(padded, first_col, part_rows, 1)
    outgoing = column_part[sources].reshape(experts, capacity, part_rows)
    landed = lax.all_to_all(outgoing, "ep", split_axis=0, concat_axis=0, tiled=True)
    portion = lax.all_gather(landed, "tp", axis=2, tiled=True)
    columns = portion.reshape(slots_all, portion.shape[2])
    gate_act = jnp.dot(columns, gate_w, preferred_element_type=jnp.float32)
    up_act = jnp.dot(columns, up_w, preferred_element_type=jnp.float32)
    hidden = (jax.nn.silu(gate_act) * up_act).astype(jnp.bfloat16)
    dense_gate_act = jnp.dot(normed, dense_gate_w, preferred_element_type=jnp.float32)
    dense_up_act = jnp.dot(normed, dense_up_w, preferred_element_type=jnp.float32)
    dense_hidden = (jax.nn.silu(dense_gate_act) * dense_up_act).astype(jnp.bfloat16)
    dense_out = lax.psum_scatter(
        transposed_term(dense_hidden, dense_down_w).astype(jnp.bfloat16),
        "tp",
        scatter_dimension=0,
        tiled=True,
    ).astype(jnp.float32)
    expert_out = lax.psum_scatter(
        transposed_term(hidden, down_w).astype(jnp.bfloat16), "tp", scatter_dimension=0, tiled=True
    )
    expert_half = expert_out.reshape(part_rows, experts, capacity)
    returned = lax.all_to_all(expert_half, "ep", split_axis=1, concat_axis=1, tiled=True).reshape(
        part_rows, slots_all
    )
    picked = (
        jnp.take(returned, places, axis=1).astype(jnp.float32).reshape(part_rows, group_tokens, 2)
    )
    routed = jnp.sum(picked * routing_weight[None, :, :], axis=2)
    gate_factor = jax.nn.sigmoid(dense_gate)[:, None]
    return (routed + gate_factor * dense_out).T.astype(jnp.bfloat16)


BF = jnp.bfloat16
F32 = jnp.float32


def silu_mul(gate_act, up_act):
    return (gate_act / (1.0 + jnp.exp(-gate_act)) * up_act).astype(BF)


def dot_t(rows, weights):
    return lax.dot_general(rows, weights, (((1,), (1,)), ((), ())), preferred_element_type=F32)


SOURCES = ((1, 2, 3), (3, 2, 0), (0, 1, 3), (2, 1, 0))
TARGETS = ((2, 3, 1), (0, 2, 3), (3, 1, 0), (1, 0, 2))
SCHEDULE = (
    "G10", "N", "G11", "H0", "X1", "C1", "D", "Y1", "G30", "W", "S1", "P00", "G31",
    "K1", "P01", "L1", "G20", "K3", "X3", "Y3", "C3", "G21", "H1", "A00", "S3", "P10",
    "K2", "X2", "L3", "C2", "P11", "Y2", "A10", "A11", "S2", "H3", "P30", "P31", "L2",
    "F1", "E1", "A30", "A31", "H2", "P20", "J1", "P21", "E3", "I1", "A20", "F3", "A21",
    "I3", "E2", "F2", "J3", "A01", "F0", "I2", "E0", "J2", "I0", "J0", "R3", "R1", "R2",
)


def fused_kernel(
    tok_hbm,
    gain_hbm,
    ids_hbm,
    rw_hbm,
    gw_hbm,
    uw_hbm,
    dw_hbm,
    dg_hbm,
    du_hbm,
    dd_hbm,
    dgate_hbm,
    out_ref,
    tok_ref,
    gain_ref,
    ids_ref,
    rw_ref,
    gw,
    uw,
    dw,
    dgu,
    dd,
    factor,
    normed,
    slot_row,
    slot_col,
    weight_col,
    gates,
    zsend,
    xbuf,
    hid_l,
    hid_c,
    dhid,
    part_l,
    part_c,
    r0_l,
    r0_c,
    r1a_l,
    r1b_l,
    r1a_c,
    r1b_c,
    r2a_l,
    r2b_l,
    r2a_c,
    r2b_c,
    fin,
    ret,
    chosen,
    scale_col,
    total,
    wsem,
    zsem,
    rsem,
    sems,
):
    me = lax.axis_index("ep")
    tp = lax.axis_index("tp")
    core, xx, yy = tp % 2, (tp // 2) % 2, tp // 4
    group, width = tok_ref.shape
    cols = out_ref.shape[1]
    rounds, cap = zsend.shape[:2]
    ffp = gw.shape[0]
    dsp = dd.shape[0]
    half = cap // 2
    mesh_id = pl.DeviceIdType.MESH
    to_core, to_x, to_y = 1, 2, 4

    def peer(flip):
        bits = (core + flip % 2) % 2, (xx + flip // 2 % 2) % 2, (yy + flip // 4) % 2
        return bits[2] * 4 + bits[1] * 2 + bits[0]

    place_value = (1 + 3 * (me % 2)) * (1 + 15 * (me // 2))

    def lookup(row):
        return sum(value * 4**plane for plane, value in enumerate(row)) // place_value % 4

    def source(slot):
        return lookup([row[slot - 1] for row in SOURCES])

    def slot_at(other):
        return lookup([SOURCES[q].index(p) for p, q in enumerate(other)])

    barrier = pltpu.get_barrier_semaphore()
    for flip in range(1, 8):
        pl.semaphore_signal(barrier, 1, device_id=(me, peer(flip)), device_id_type=mesh_id)
    for j in range(1, rounds + 1):
        pl.semaphore_signal(
            barrier, 1, device_id=((me + j) % 4, peer(to_core)), device_id_type=mesh_id
        )

    loads = {
        "ids": pltpu.make_async_copy(ids_hbm, ids_ref, wsem.at[6]),
        "gain": pltpu.make_async_copy(gain_hbm, gain_ref, wsem.at[8]),
        "rw": pltpu.make_async_copy(rw_hbm, rw_ref, wsem.at[9]),
        "dgate": pltpu.make_async_copy(dgate_hbm, gates.at[tp], wsem.at[10]),
        "g": pltpu.make_async_copy(gw_hbm.at[0], gw, wsem.at[0]),
        "u": pltpu.make_async_copy(uw_hbm.at[0], uw, wsem.at[1]),
        "dg": pltpu.make_async_copy(dg_hbm, dgu.at[:, pl.ds(0, dsp)], wsem.at[2]),
        "du": pltpu.make_async_copy(du_hbm, dgu.at[:, pl.ds(dsp, dsp)], wsem.at[3]),
        "d": pltpu.make_async_copy(dw_hbm.at[0], dw, wsem.at[4]),
        "dd": pltpu.make_async_copy(dd_hbm, dd, wsem.at[5]),
    }
    step = group // 4
    for i in range(4):
        rows = pl.ds(i * step, step)
        copy = pltpu.make_async_copy(tok_hbm.at[rows], tok_ref.at[rows], wsem.at[11 + i])
        loads = {"tok%d" % i: copy, **loads}
    loads = {"ids": loads.pop("ids"), **{"tok%d" % i: loads["tok%d" % i] for i in range(4)}, **loads}
    for load in loads.values():
        load.start()

    def need(*names):
        for name in names:
            if name in loads:
                loads.pop(name).wait()

    started, expected = [], {}

    def transfer(src, dst, send_sem, recv_sem, target):
        return pltpu.make_async_remote_copy(
            src_ref=src,
            dst_ref=dst,
            send_sem=send_sem,
            recv_sem=recv_sem,
            device_id=target,
            device_id_type=mesh_id,
        )

    def send(name, src, dst, target):
        n = len(started)
        copy = transfer(src, dst, sems.at[0, n], sems.at[1, n], target)
        copy.start()
        started.append(copy)
        expected[name] = copy

    def got(*names):
        for name in names:
            if expected[name] is not None:
                expected[name].wait_recv()
                expected[name] = None

    def hop(sem, src, dst, number, landing, h, plane):
        rows = tops[h]
        copy = transfer(
            src.at[number, rows],
            dst(landing, rows, tp),
            sem.at[0, number, h],
            sem.at[1, landing, h],
            (plane, peer(to_core)),
        )
        copy.start()
        started.append(copy)

    def z_place(slot, rows, part):
        return xbuf.at[slot, rows, span(part)]

    def r_place(slot, rows, part):
        return ret.at[slot, rows]

    def at_tp(flip):
        return (me, peer(flip))

    tops = {0: pl.ds(0, half), 1: pl.ds(half, half)}

    def span(slice_no):
        return pl.ds(pl.multiple_of(slice_no * cols, cols), cols)

    number = lax.broadcasted_iota(jnp.int32, (128, group), 0)
    earlier = jnp.where(
        lax.broadcasted_iota(jnp.int32, (group, group), 0)
        < lax.broadcasted_iota(jnp.int32, (group, group), 1),
        1.0,
        0.0,
    ).astype(BF)
    need("ids")
    id0, id1 = ids_ref[0:1, :], ids_ref[1:2, :]
    named = (id0 == number) | (id1 == number)
    marks = jnp.where(named, 1.0, 0.0).astype(BF)
    count = jnp.dot(marks, earlier, preferred_element_type=F32)
    slots = jnp.where(named, count, -1.0)
    slot_row[...] = slots

    for i in range(4):
        need("tok%d" % i)
        rows = pl.ds(i * step, step)
        values = tok_ref[rows, :].astype(F32)
        mean = jnp.sum(values * values, axis=1, keepdims=True) * (1.0 / width)
        factor[rows, :] = jnp.broadcast_to(lax.rsqrt(mean + EPSILON), (step, 128))

    def pick(e):
        row = slot_row[pl.ds(e, 1), :].astype(jnp.int32)
        where = lax.broadcasted_iota(jnp.int32, (cap, group), 0)
        return jnp.where(row == where, 1.0, 0.0).astype(BF)

    need("gain")
    own = (tok_ref[:, span(tp)].astype(F32) * factor[:, 0:1] * gain_ref[:, span(tp)]).astype(BF)
    for n in range(rounds):
        targets = [row[n] for row in TARGETS]
        plane = lookup(targets)
        zsend[n] = jnp.dot(pick(plane), own, preferred_element_type=F32).astype(BF)
        if n == 0:
            pl.semaphore_wait(barrier, 7 + rounds)
        for h in tops:
            hop(zsem, zsend, z_place, n, slot_at(targets), h, plane)
    for n in range(rounds):
        for h, rows in tops.items():
            for kind, sem, src, place in (("z", zsem, zsend, z_place), ("r", rsem, fin, r_place)):
                landed = place(n, rows, peer(to_core))
                expected[kind, n + 1, h] = transfer(
                    src.at[n, rows], landed, sem.at[0, n, h], sem.at[1, n, h], at_tp(to_core)
                )
    need("dgate", "rw")
    for flip in range(1, 8):
        send(("gate", flip), gates.at[tp], gates.at[tp], at_tp(flip))

    weights = jnp.where(id0 == number, rw_ref[0:1, :], 0.0) + jnp.where(id1 == number, rw_ref[1:2, :], 0.0)
    slot_col[...] = slots.T
    weight_col[...] = weights.T
    lane = lax.broadcasted_iota(jnp.int32, (group, 128), 1)

    def weight_of(e):
        return jnp.sum(jnp.where(lane == e, weight_col[...], 0.0), axis=1, keepdims=True)

    def norm_all():
        gain = gain_ref[...]

        def body(i, carry):
            rows = pl.ds(pl.multiple_of(i * 32, 32), 32)
            values = tok_ref[rows, :].astype(F32)
            normed[rows, :] = (values * factor[rows, 0:1] * gain).astype(BF)
            return carry

        lax.fori_loop(0, group // 32, body, 0)

    def forward(name, j, rows, slice_flip, flip):
        ref = xbuf.at[j - 1, rows, span(peer(slice_flip))]
        send((name, j), ref, ref, at_tp(flip))

    everything = pl.ds(0, cap)

    def gather_start(j, h):
        got(("z", j, h))
        forward("x%d" % h, j, tops[h], to_core, to_x + to_core)
        forward("y%d" % h, j, tops[h], to_core, to_y + to_core)

    def gather_core(j):
        forward("c", j, everything, to_core, to_core)

    def gather_relay_x(j):
        got(("x0", j))
        forward("xy", j, tops[0], to_x, to_y + to_core)

    def gather_relay_y(j):
        got(("y1", j))
        forward("yx", j, tops[1], to_y, to_x + to_core)

    def gather_share(j):
        got(("x0", j), ("x1", j))
        forward("xc", j, everything, to_x, to_core)
        got(("y0", j), ("y1", j))
        forward("yc", j, everything, to_y, to_core)

    def gather_last(j):
        got(("xy", j))
        forward("xyc", j, tops[0], 7, to_core)
        got(("yx", j))
        forward("yxc", j, tops[1], 7, to_core)

    def hidden(b):
        need("g", "u")
        if b:
            got(*[(name, b) for name in ("c", "xc", "yc", "xyc", "yxc")])
        rows = xbuf[b - 1] if b else normed[...]
        value = silu_mul(dot_t(rows, gw[...]), dot_t(rows, uw[...]))
        if b:
            hid_c[b - 1] = value
        else:
            hid_l[...] = value

    def local_scale():
        scale_col[rounds] = jnp.broadcast_to(weight_of(me), (group, 128))

    def dense_hidden():
        need("dg", "du")
        both = jnp.dot(normed[...], dgu[...], preferred_element_type=F32)
        dhid[...] = silu_mul(both[:, :dsp], both[:, dsp:])

    def rs_refs(b):
        if b == 0:
            return part_l, r0_l, r1a_l, r1b_l, r2a_l, r2b_l
        return tuple(r.at[b - 1] for r in (part_c, r0_c, r1a_c, r1b_c, r2a_c, r2b_c))

    def halves(b):
        h = (cap if b else group) // 2
        return pl.ds(0, h), pl.ds(h, h)

    def partial(b, mine):
        need("d", "dd")
        half_no = 0 if mine else 1
        swap = half_no + (1 if b else 0)
        part, r0 = rs_refs(b)[:2]
        if b == 0:
            scale = scale_col[rounds][:, 0:1]
            got(*[("gate", flip) for flip in range(1, 8)])
        corners = ((1 - yy, 1 - xx), (yy, 1 - xx), (1 - yy, xx), (yy, xx))
        for (y, x), odd in zip(corners, (0, 1, 1, 0)):
            k = 4 * y + 2 * x + (core + odd + swap) % 2
            if b:
                value = jnp.dot(hid_c[b - 1], dw[:, span(k)], preferred_element_type=F32)
            else:
                side = jnp.dot(dhid[...], dd[:, span(k)], preferred_element_type=F32)
                value = jnp.dot(hid_l[...], dw[:, span(k)], preferred_element_type=F32)
                value = scale * value + jax.nn.sigmoid(gates[k]) * side
            part[half_no, y, x] = value.astype(BF)
        if not mine:
            for q, (y, x) in enumerate(corners):
                send(("r0", q, b), part.at[half_no, y, x], r0.at[y, x], at_tp(to_core))

    def add(dst, index, other):
        dst[index] = (dst[index].astype(F32) + other.astype(F32)).astype(BF)

    def scatter_one(b, late):
        part, r0, r1a, r1b = rs_refs(b)[:4]
        top, bottom = halves(b)
        if not late:
            got(("r0", 0, b))
            add(part, (0, 1 - yy, 1 - xx), r0[1 - yy, 1 - xx])
            send(("a0", b), part.at[0, 1 - yy, 1 - xx, top], r1a.at[1 - yy], at_tp(to_x + to_core))
            send(("b0", b), part.at[0, 1 - yy, 1 - xx, bottom], r1b.at[1 - xx], at_tp(to_y + to_core))
        else:
            got(("r0", 1, b))
            add(part, (0, yy, 1 - xx), r0[yy, 1 - xx])
            send(("a1", b), part.at[0, yy, 1 - xx, top], r1a.at[yy], at_tp(to_x + to_core))
            got(("r0", 2, b))
            add(part, (0, 1 - yy, xx), r0[1 - yy, xx])
            send(("b1", b), part.at[0, 1 - yy, xx, bottom], r1b.at[xx], at_tp(to_y + to_core))

    def scatter_two_a(b):
        part, r0, r1a, r1b, r2a, r2b = rs_refs(b)
        top, bottom = halves(b)
        got(("a0", b))
        add(part, (0, 1 - yy, xx, top), r1a[1 - yy])
        send(("a2", b), part.at[0, 1 - yy, xx, top], r2a, at_tp(to_y + to_core))

    def scatter_two_b(b):
        part, r0, r1a, r1b, r2a, r2b = rs_refs(b)
        top, bottom = halves(b)
        got(("b0", b))
        add(part, (0, yy, 1 - xx, bottom), r1b[1 - xx])
        send(("b2", b), part.at[0, yy, 1 - xx, bottom], r2b, at_tp(to_x + to_core))

    def finish(b, h, value):
        rows = halves(b)[h]
        if b == 0:
            total[rows, :] = value
        else:
            fin[b - 1, rows, :] = value.astype(BF)
            sources = [row[b - 1] for row in SOURCES]
            hop(rsem, fin, r_place, b - 1, slot_at(sources), h, source(b))

    def scatter_three_a(b):
        part, r0, r1a, r1b, r2a, r2b = rs_refs(b)
        rows = halves(b)[0]
        got(("r0", 3, b), ("a1", b), ("a2", b))
        mine = part[0, yy, xx, rows].astype(F32) + r0[yy, xx, rows].astype(F32)
        finish(b, 0, mine + r1a[yy].astype(F32) + r2a[...].astype(F32))

    def scatter_three_b(b):
        part, r0, r1a, r1b, r2a, r2b = rs_refs(b)
        rows = halves(b)[1]
        got(("r0", 3, b), ("b1", b), ("b2", b))
        mine = part[0, yy, xx, rows].astype(F32) + r0[yy, xx, rows].astype(F32)
        finish(b, 1, mine + r1b[xx].astype(F32) + r2b[...].astype(F32))

    def prepare(j):
        e = source(j)
        slot = jnp.sum(jnp.where(lane == e, slot_col[...], 0.0), axis=1, keepdims=True).astype(jnp.int32)
        where = lax.broadcasted_iota(jnp.int32, (group, cap), 1)
        chosen[j - 1] = jnp.where(slot == where, 1.0, 0.0).astype(BF)
        scale_col[j - 1] = jnp.broadcast_to(weight_of(e), (group, 128))

    def returned(j):
        got(("r", j, 0), ("r", j, 1))
        rows = jnp.dot(chosen[j - 1], ret[j - 1], preferred_element_type=F32)
        value = total[...] + scale_col[j - 1][:, 0:1] * rows
        if ("R%d" % j) == SCHEDULE[-1]:
            out_ref[...] = value.astype(BF)
        else:
            total[...] = value

    steps = {
        "N": norm_all,
        "G": gather_start,
        "C": gather_core,
        "X": gather_relay_x,
        "Y": gather_relay_y,
        "S": gather_share,
        "L": gather_last,
        "H": hidden,
        "W": local_scale,
        "D": dense_hidden,
        "P": partial,
        "A": scatter_one,
        "E": scatter_two_a,
        "F": scatter_two_b,
        "I": scatter_three_a,
        "J": scatter_three_b,
        "K": prepare,
        "R": returned,
    }
    for word in SCHEDULE:
        steps[word[0]](*[int(digit) for digit in word[1:]])
    for copy in started:
        copy.wait_send()


def fused_local(
    tokens,
    norm_gain,
    expert_ids,
    routing_weight,
    expert_gate,
    expert_up,
    expert_down,
    dense_gate_w,
    dense_up_w,
    dense_down_w,
    dense_gate,
):
    experts = lax.axis_size("ep")
    parts = lax.axis_size("tp")
    group, width = tokens.shape
    cap = 3 * group // experts
    cols = width // parts
    ffp = expert_gate.shape[2]
    dsp = dense_gate_w.shape[1]
    rounds = experts - 1
    vmem, hbm = pl.BlockSpec(memory_space=pltpu.VMEM), pl.BlockSpec(memory_space=pl.ANY)
    dma = pltpu.SemaphoreType.DMA
    half, ghalf = cap // 2, group // 2
    return pl.pallas_call(
        fused_kernel,
        out_shape=pltpu.VMEM((group, cols), BF),
        in_specs=[hbm] * 11,
        out_specs=vmem,
        scratch_shapes=[
            pltpu.VMEM((group, width), BF),
            pltpu.VMEM((1, width), F32),
            pltpu.VMEM((2, group), jnp.int32),
            pltpu.VMEM((2, group), F32),
            pltpu.VMEM((ffp, width), BF),
            pltpu.VMEM((ffp, width), BF),
            pltpu.VMEM((ffp, width), BF),
            pltpu.VMEM((width, 2 * dsp), BF),
            pltpu.VMEM((dsp, width), BF),
            pltpu.VMEM((group, 128), F32),
            pltpu.VMEM((group, width), BF),
            pltpu.VMEM((128, group), F32),
            pltpu.VMEM((group, 128), F32),
            pltpu.VMEM((group, 128), F32),
            pltpu.VMEM((parts, 1, cols), F32),
            pltpu.VMEM((rounds, cap, cols), BF),
            pltpu.VMEM((rounds, cap, width), BF),
            pltpu.VMEM((group, ffp), BF),
            pltpu.VMEM((rounds, cap, ffp), BF),
            pltpu.VMEM((group, dsp), BF),
            pltpu.VMEM((2, 2, 2, group, cols), BF),
            pltpu.VMEM((rounds, 2, 2, 2, cap, cols), BF),
            pltpu.VMEM((2, 2, group, cols), BF),
            pltpu.VMEM((rounds, 2, 2, cap, cols), BF),
            pltpu.VMEM((2, ghalf, cols), BF),
            pltpu.VMEM((2, ghalf, cols), BF),
            pltpu.VMEM((rounds, 2, half, cols), BF),
            pltpu.VMEM((rounds, 2, half, cols), BF),
            pltpu.VMEM((ghalf, cols), BF),
            pltpu.VMEM((ghalf, cols), BF),
            pltpu.VMEM((rounds, half, cols), BF),
            pltpu.VMEM((rounds, half, cols), BF),
            pltpu.VMEM((rounds, cap, cols), BF),
            pltpu.VMEM((rounds, cap, cols), BF),
            pltpu.VMEM((rounds, group, cap), BF),
            pltpu.VMEM((rounds + 1, group, 128), F32),
            pltpu.VMEM((group, cols), F32),
            dma((15,)),
            dma((2, rounds, 2)),
            dma((2, rounds, 2)),
            dma((2, 92)),
        ],
        compiler_params=pltpu.CompilerParams(
            collective_id=0, has_side_effects=True, vmem_limit_bytes=56 * 1024 * 1024
        ),
        name="routed_layer",
    )(
        tokens,
        norm_gain[None, :],
        expert_ids.T,
        routing_weight.T,
        jnp.swapaxes(expert_gate, 1, 2),
        jnp.swapaxes(expert_up, 1, 2),
        expert_down,
        dense_gate_w,
        dense_up_w,
        dense_down_w,
        dense_gate[None, :],
    )


def local(*args):
    experts, parts = lax.axis_size("ep"), lax.axis_size("tp")
    group, width = args[0].shape
    fits = (
        experts == 4
        and parts == 8
        and width % (128 * parts) == 0
        and group % 128 == 0
        and (3 * group // experts) % 32 == 0
        and args[7].shape[1] % 128 == 0
        and args[4].shape[2] % 16 == 0
    )
    return (fused_local if fits else plain_local)(*args)


def solution(mesh):
    return jax.shard_map(
        local,
        mesh=mesh,
        in_specs=(
            P("ep", None),
            P(),
            P("ep", None),
            P("ep", None),
            P("ep", None, "tp"),
            P("ep", None, "tp"),
            P("ep", "tp", None),
            P(None, "tp"),
            P(None, "tp"),
            P("tp", None),
            P("tp"),
        ),
        out_specs=P("ep", "tp"),
        check_vma=False,
    )
```
